128 devices in a mesh: sp: 32 (over z, y, core), tp: 4 (over x).
Axes of the slice: x: 4, y: 4, z: 4, core: 2. Of those that a mesh axis runs over, the one named last changes fastest.
Arguments:
- residual_in: bfloat16 [32768, 2048], P(('sp', 'tp')), may hold values from -6 to 6
- queries: bfloat16 [32768, 2048], P('sp', 'tp'), may hold values from -200 to 200, as said below
- keys_values: bfloat16 [2, 32768, 1024], P(None, 'sp', 'tp'), may hold values from -6 to 6
- sink_logit: float32 [32], P('tp'), may hold values from -2 to 6
- out_weight: bfloat16 [2048, 2048], P('tp'), may hold values from -2 to 2
- norm1_gain: float32 [2048], replicated, may hold values from 0.1 to 1.9
- norm1_bias: float32 [2048], replicated, may hold values from -3 to 3
- up_weight: bfloat16 [2048, 8192], P('sp', 'tp'), may hold values from -0.125 to 0.125
- down_weight: bfloat16 [8192, 2048], P('tp', 'sp'), may hold values from -0.0625 to 0.0625
- norm2_gain: float32 [2048], replicated, may hold values from 0.1 to 1.9
- norm2_bias: float32 [2048], replicated, may hold values from -3 to 3
Outputs:
- stream_out: bfloat16 [32768, 2048], P(('sp', 'tp'))
The draws below stay inside these ranges and needn't reach their ends.
Inputs may be any that keep to these rules, and one draw needn't show every extreme that they name: `queries`: of order one mostly; some rows may be large multiples of a nearby key row.
All inputs are finite; a program needn't handle non-finite values.
Results may differ from the reference program's by a relative error of at most 0.014.
Values may be sent and summed in bfloat16 or wider, within the bound.
No kernel may reach another device: no remote copies, remote signals or barrier semaphores. Data moves between devices by JAX's collectives and lax.ppermute only.
A program may use at most 128 MiB of HBM per device.

```python
import jax
import jax.numpy as jnp
from jax import lax

D = 2048
HEADS = 32
KV_HEADS = 16
HEAD_DIM = 64
FF = 8192
WINDOW = 128
TOK_DEV = 1024
TOKENS = 32768
N_TP = 4


def joint_draw(key):
    query = jnp.clip(jax.random.normal(jax.random.fold_in(key, 11), (TOKENS, HEADS * HEAD_DIM), jnp.float32), -5.0, 5.0)
    pairs = jnp.clip(jax.random.normal(jax.random.fold_in(key, 12), (2, TOKENS, KV_HEADS * HEAD_DIM), jnp.float32), -5.0, 5.0)
    return (query, pairs)


def draw_queries(key, part):
    return joint_draw(key)[0].astype(jnp.bfloat16)


def draw_keys_values(key, part):
    return joint_draw(key)[1].astype(jnp.bfloat16)


def levels(key, extent, split, low, top_value):
    level = 1.0
    for dim, shards_of in split:
        heights = jax.random.uniform(jax.random.fold_in(jax.random.fold_in(key, 6), dim), (shards_of,), jnp.float32, low / len(split), top_value / len(split))
        level = level * jnp.repeat(jnp.exp(heights), extent[dim] // shards_of).reshape((-1,) + (1,) * (len(extent) - 1 - dim))
    return level


def noise(rng, extent, width, most, split=(), kind=jnp.bfloat16):
    factor_of = levels(rng, extent, split, -0.22, 0.18) if split else 1.0
    values = jax.random.normal(rng, extent, jnp.float32) * width * factor_of
    return jnp.minimum(jnp.maximum(values, -most), most).astype(kind)


def setup_inputs(seed: int = 0) -> dict:
    splits = jax.random.split(jax.random.key(seed), 12)
    residual_in = noise(splits[0], (TOKENS, D), 1.0, 6.0, ((0, 128),))
    queries = draw_queries(jax.random.fold_in(splits[11], 71), 0)
    keys_values = draw_keys_values(jax.random.fold_in(splits[11], 71), 0)
    sink_logit = jnp.clip(-2.0 + 8.0 * jax.random.uniform(splits[3], (HEADS,), jnp.float32) ** levels(splits[3], (HEADS,), ((0, 4),), -0.2, 0.2), -2.0, 6.0)
    out_weight = noise(splits[4], (HEADS * HEAD_DIM, D), (6 * (HEADS * HEAD_DIM) ** -0.5), 2.0, ((0, 4),))
    norm1_gain = jnp.clip(1.0 + 0.18 * jax.random.normal(splits[5], (D,), jnp.float32), 0.1, 1.9)
    norm1_bias = noise(splits[6], (D,), 0.3, 3.0, (), jnp.float32)
    up_weight = noise(splits[7], (D, FF), D ** -0.5, 0.125, ((0, 32), (1, 4)))
    down_weight = noise(splits[8], (FF, D), FF ** -0.5, 0.0625, ((0, 4), (1, 32)))
    norm2_gain = jnp.clip(1.0 + 0.18 * jax.random.normal(splits[9], (D,), jnp.float32), 0.1, 1.9)
    norm2_bias = noise(splits[10], (D,), 0.3, 3.0, (), jnp.float32)
    return dict(residual_in=residual_in, queries=queries, keys_values=keys_values, sink_logit=sink_logit, out_weight=out_weight, norm1_gain=norm1_gain, norm1_bias=norm1_bias, up_weight=up_weight, down_weight=down_weight, norm2_gain=norm2_gain, norm2_bias=norm2_bias)


def norm_rows(values, gain, bias):
    mean = lax.optimization_barrier(jnp.mean(values, axis=-1, keepdims=True))
    centred = values - mean
    variance = lax.optimization_barrier(jnp.mean(centred * centred, axis=-1, keepdims=True))
    return (centred * lax.rsqrt(variance + 1e-06) * gain + bias).astype(jnp.bfloat16)

def reference(residual_in, queries, keys_values, sink_logit, out_weight, norm1_gain, norm1_bias, up_weight, down_weight, norm2_gain, norm2_bias):
    block = min(512, TOK_DEV)
    span = block + 2 * WINDOW
    group = HEADS // KV_HEADS
    padded = jnp.pad(keys_values, ((0, 0), (WINDOW, WINDOW), (0, 0)))
    sink = sink_logit.reshape(KV_HEADS, group, 1, 1)

    def one_block(index):
        start = (index * block).astype(jnp.int32)
        query = lax.dynamic_slice_in_dim(queries, start, block, 0).astype(jnp.float32).reshape(block, KV_HEADS, group, HEAD_DIM)
        keys = lax.dynamic_slice_in_dim(padded[0], start, span, 0).astype(jnp.float32).reshape(span, KV_HEADS, HEAD_DIM)
        values = lax.dynamic_slice_in_dim(padded[1], start, span, 0).astype(jnp.float32).reshape(span, KV_HEADS, HEAD_DIM)
        scores = jnp.einsum('qhgd,khd->hgqk', query, keys) * HEAD_DIM ** (-0.5)
        query_pos = start + jnp.arange(block, dtype=jnp.int32)
        key_pos = start - WINDOW + jnp.arange(span, dtype=jnp.int32)
        valid = (jnp.abs(key_pos[None, :] - query_pos[:, None]) <= WINDOW) & (key_pos[None, :] >= 0) & (key_pos[None, :] < TOKENS)
        scores = jnp.where(valid, scores, -jnp.inf)
        top = jnp.maximum(lax.optimization_barrier(jnp.max(scores, axis=-1, keepdims=True)), sink)
        expd = jnp.exp(scores - top)
        total = lax.optimization_barrier(jnp.sum(expd, axis=-1, keepdims=True)) + jnp.exp(sink - top)
        weights = lax.optimization_barrier((expd / total).astype(jnp.bfloat16)).astype(jnp.float32)
        mixed = jnp.einsum('hgqk,khd->qhgd', weights, values)
        return mixed.reshape(block, HEADS * HEAD_DIM).astype(jnp.bfloat16)
    attended = lax.map(one_block, jnp.arange(TOKENS // block, dtype=jnp.int32)).reshape(TOKENS, HEADS * HEAD_DIM)
    head_cols = HEADS * HEAD_DIM // N_TP
    projected = jnp.zeros((TOKENS, D), jnp.float32)
    for part in range(N_TP):
        term = jnp.dot(attended[:, part * head_cols:(part + 1) * head_cols], out_weight[part * head_cols:(part + 1) * head_cols], preferred_element_type=jnp.float32)
        projected = projected + term.astype(jnp.bfloat16).astype(jnp.float32)
    first = norm_rows(residual_in.astype(jnp.float32) + projected, norm1_gain, norm1_bias)
    hidden = jnp.dot(first, up_weight, preferred_element_type=jnp.float32)
    activation = jnp.square(jnp.maximum(hidden, 0.0)).astype(jnp.bfloat16)
    unit_cols = FF // N_TP
    branch = jnp.zeros((TOKENS, D), jnp.float32)
    for part in range(N_TP):
        term = jnp.dot(activation[:, part * unit_cols:(part + 1) * unit_cols], down_weight[part * unit_cols:(part + 1) * unit_cols], preferred_element_type=jnp.float32)
        branch = branch + term.astype(jnp.bfloat16).astype(jnp.float32)
    return norm_rows(first.astype(jnp.float32) + branch, norm2_gain, norm2_bias)
```

```python
import functools

import jax
import jax.numpy as jnp
from jax import lax
from jax.experimental import pallas as pl
from jax.experimental.pallas import tpu as pltpu
from jax.sharding import PartitionSpec as P

HEAD_DIM = 64
WINDOW = 128
LANES = 128
NEG = -1e30


def shift(value, axis, step):
    devices = lax.axis_size(axis)
    return lax.ppermute(value, axis, [(i, (i + step) % devices) for i in range(devices)])


def halo(shard, axis, width):
    devices, length = (lax.axis_size(axis), shard.shape[1])
    up = [(i, i + 1) for i in range(devices - 1)]
    down = [(j, i) for i, j in up]
    before = lax.ppermute(shard[:, length - width :], axis, up)
    after = lax.ppermute(shard[:, :width], axis, down)
    return jnp.concatenate([before, shard, after], axis=1)


def attend_kernel(place, sink, q_ref, kv_ref, w_ref, out_ref, *, rel, n_sp, tok_rows):
    step = pl.program_id(0)
    rows = q_ref.shape[0]
    quarter = (place[0] + rel(step)) % (tok_rows // rows)
    blocks = rows // WINDOW
    pairs = q_ref.shape[1] // LANES
    row = lax.broadcasted_iota(jnp.int32, (2 * WINDOW, WINDOW), 0) % WINDOW
    col = lax.broadcasted_iota(jnp.int32, (2 * WINDOW, WINDOW), 1)
    low = lax.broadcasted_iota(jnp.int32, (WINDOW, LANES), 1) < HEAD_DIM
    upper = lax.broadcasted_iota(jnp.int32, (2 * WINDOW, 1), 0) < WINDOW
    ones = jnp.ones((3 * WINDOW, LANES), jnp.bfloat16)
    finished = []
    for block in range(blocks):
        index = quarter * blocks + block
        at_start = jnp.where((place[1] == 0) & (index == 0), 4 * WINDOW, 0)
        at_end = jnp.where((place[1] == n_sp - 1) & (index == tok_rows // WINDOW - 1), 4 * WINDOW, 0)
        before_ok = col - row >= at_start
        after_ok = row - col >= at_end
        start = pl.multiple_of(index * WINDOW, WINDOW)
        mixed = []
        for pair in range(pairs):
            tile, half = (pair // 2, pair % 2)
            lanes = slice(tile * LANES, (tile + 1) * LANES)
            query = q_ref[block * WINDOW : (block + 1) * WINDOW, pair * LANES : (pair + 1) * LANES]
            query = query.astype(jnp.float32) * HEAD_DIM**-0.5
            turned = pltpu.roll(query, HEAD_DIM, 1)
            if half == 0:
                both = (jnp.where(low, query, 0.0), jnp.where(low, turned, 0.0))
            else:
                both = (jnp.where(low, 0.0, turned), jnp.where(low, 0.0, query))
            query = jnp.concatenate(both, axis=0).astype(jnp.bfloat16)
            keys = kv_ref[0, pl.ds(start, 3 * WINDOW), lanes]
            values = kv_ref[1, pl.ds(start, 3 * WINDOW), lanes]
            scores = lax.dot_general(
                query, keys, (((1,), (1,)), ((), ())), preferred_element_type=jnp.float32
            )
            before = jnp.where(before_ok, scores[:, :WINDOW], NEG)
            middle = scores[:, WINDOW : 2 * WINDOW]
            after = jnp.where(after_ok, scores[:, 2 * WINDOW :], NEG)
            sink_col = jnp.where(upper, sink[2 * pair], sink[2 * pair + 1])
            top = jnp.max(
                jnp.maximum(jnp.maximum(before, after), middle), axis=-1, keepdims=True
            )
            top = jnp.maximum(top, sink_col)
            expd = jnp.concatenate(
                [jnp.exp(part - top).astype(jnp.bfloat16) for part in (before, middle, after)],
                axis=1,
            )
            summed = jnp.dot(
                expd,
                jnp.concatenate([values, ones], axis=1),
                preferred_element_type=jnp.float32,
            )
            result = summed[:, :LANES] / (summed[:, LANES:] + jnp.exp(sink_col - top))
            first, second = (result[:WINDOW], result[WINDOW:])
            if half == 0:
                second = pltpu.roll(second, HEAD_DIM, 1)
            else:
                first = pltpu.roll(first, HEAD_DIM, 1)
            mixed.append(jnp.where(low, first, second).astype(jnp.bfloat16))
        finished.append(jnp.concatenate(mixed, axis=1))
    attended = jnp.concatenate(finished, axis=0)
    out_ref[...] = jnp.dot(attended, w_ref[...], preferred_element_type=jnp.float32).astype(
        jnp.bfloat16
    )


def attend(place, sink, queries, padded, out_weight, steps, rel, n_tp, n_sp):
    tok_rows, width = queries.shape
    rows = tok_rows // n_tp
    cols = out_weight.shape[1]
    return pl.pallas_call(
        functools.partial(attend_kernel, rel=rel, n_sp=n_sp, tok_rows=tok_rows),
        grid_spec=pltpu.PrefetchScalarGridSpec(
            num_scalar_prefetch=2,
            grid=(steps,),
            in_specs=[
                pl.BlockSpec((rows, width), lambda i, place, sink: ((place[0] + rel(i)) % n_tp, 0)),
                pl.BlockSpec(padded.shape, lambda i, place, sink: (0, 0, 0)),
                pl.BlockSpec(out_weight.shape, lambda i, place, sink: (0, 0)),
            ],
            out_specs=pl.BlockSpec((rows, cols), lambda i, place, sink: (i, 0)),
        ),
        out_shape=jax.ShapeDtypeStruct((steps * rows, cols), jnp.bfloat16),
        name="attend",
    )(place, sink, queries, padded, out_weight)


def norm_kernel(*refs):
    gain, bias, out_ref = refs[-3:]
    values = refs[0][...].astype(jnp.float32)
    for ref in refs[1:-3]:
        values = values + ref[...].astype(jnp.float32)
    width = values.shape[1]
    mean = jnp.sum(values, axis=-1, keepdims=True) * (1.0 / width)
    centred = values - mean
    variance = jnp.sum(centred * centred, axis=-1, keepdims=True) * (1.0 / width)
    out_ref[...] = (centred * lax.rsqrt(variance + 1e-06) * gain[...] + bias[...]).astype(
        jnp.bfloat16
    )


def norm_rows(parts, gain, bias, block=64):
    rows, width = parts[0].shape
    tile = pl.BlockSpec((block, width), lambda i: (i, 0))
    line = pl.BlockSpec((1, width), lambda i: (0, 0))
    return pl.pallas_call(
        norm_kernel,
        grid=(rows // block,),
        in_specs=[tile] * len(parts) + [line, line],
        out_specs=tile,
        out_shape=jax.ShapeDtypeStruct((rows, width), jnp.bfloat16),
        name="norm",
    )(*parts, gain[None], bias[None])


def added(part, arrived, top):
    half = arrived.shape[0]
    mine = part[:half] if top else part[half:]
    total = (mine.astype(jnp.float32) + arrived.astype(jnp.float32)).astype(jnp.bfloat16)
    return jnp.concatenate([total, part[half:]] if top else [part[:half], total], axis=0)


def ring_sum(far, right, left):
    half = far.shape[0] // 2
    from_left = shift(far[:half], "tp", 1)
    from_right = shift(far[half:], "tp", -1)
    return (
        shift(added(right, from_left, True), "tp", 1),
        shift(added(left, from_right, False), "tp", -1),
    )


def feed_forward(rows, up_full, down_full):
    hidden = jnp.dot(rows, up_full, preferred_element_type=jnp.float32)
    activation = jnp.square(jnp.maximum(hidden, 0.0)).astype(jnp.bfloat16)
    return lax.dot_general(
        activation, down_full, (((1,), (1,)), ((), ())), preferred_element_type=jnp.float32
    ).astype(jnp.bfloat16)


def on_device(
    residual_in,
    queries,
    keys_values,
    sink_logit,
    out_weight,
    norm1_gain,
    norm1_bias,
    up_weight,
    down_weight,
    norm2_gain,
    norm2_bias,
):
    n_tp, n_sp = (lax.axis_size("tp"), lax.axis_size("sp"))
    up_full = lax.all_gather(up_weight, "sp", axis=0, tiled=True)
    down_full = lax.all_gather(down_weight.T, "sp", axis=0, tiled=True)
    place = jnp.where(
        jnp.arange(2, dtype=jnp.int32) == 0, lax.axis_index("tp"), lax.axis_index("sp")
    )
    padded = halo(keys_values, "sp", WINDOW)
    run = functools.partial(attend, place, sink_logit, queries, padded, out_weight)
    rows = queries.shape[0] // n_tp
    far = run(1, lambda i: 2, n_tp, n_sp)
    near = run(3, lambda i: 1 + 2 * i - i // 2, n_tp, n_sp)
    right, left, own = (near[:rows], near[rows : 2 * rows], near[2 * rows :])
    arrived = ring_sum(far, right, left)
    first = norm_rows((residual_in, own, *arrived), norm1_gain, norm1_bias)

    half = rows // 2
    of_left, of_right = (shift(first, "tp", 1), shift(first, "tp", -1))
    of_far = jnp.concatenate(
        [shift(of_left[:half], "tp", 1), shift(of_right[half:], "tp", -1)], axis=0
    )
    far = feed_forward(of_far, up_full, down_full)
    right = feed_forward(of_right, up_full, down_full)
    left = feed_forward(of_left, up_full, down_full)
    own = feed_forward(first, up_full, down_full)
    arrived = ring_sum(far, right, left)
    return norm_rows((first, own, *arrived), norm2_gain, norm2_bias)


def solution(mesh):
    return jax.shard_map(
        on_device,
        mesh=mesh,
        in_specs=(
            P(("sp", "tp"), None),
            P("sp", "tp"),
            P(None, "sp", "tp"),
            P("tp"),
            P("tp", None),
            P(),
            P(),
            P("sp", "tp"),
            P("tp", "sp"),
            P(),
            P(),
        ),
        out_specs=P(("sp", "tp"), None),
        check_vma=False,
    )
```

```python
import functools

import jax
import jax.numpy as jnp
from jax import lax
from jax.experimental import pallas as pl
from jax.experimental.pallas import tpu as pltpu
from jax.sharding import PartitionSpec as P

HEAD_DIM = 64
WINDOW = 128
LANES = 128
NEG = -1e30


def shift(value, axis, step):
    devices = lax.axis_size(axis)
    return lax.ppermute(value, axis, [(i, (i + step) % devices) for i in range(devices)])


def halo(shard, axis, width):
    devices, length = (lax.axis_size(axis), shard.shape[1])
    up = [(i, i + 1) for i in range(devices - 1)]
    down = [(j, i) for i, j in up]
    before = lax.ppermute(shard[:, length - width :], axis, up)
    after = lax.ppermute(shard[:, :width], axis, down)
    return before, after


def attend_kernel(
    place, sink, q_ref, before_ref, mid_ref, after_ref, w_ref, *refs, rel, n_sp, tok_rows
):
    *out_refs, kv_ref = refs
    step = pl.program_id(0)

    @pl.when(step == 0)
    def _():
        kv_ref[:, :WINDOW] = before_ref[...]
        kv_ref[:, WINDOW : WINDOW + tok_rows] = mid_ref[...]
        kv_ref[:, WINDOW + tok_rows :] = after_ref[...]

    rows = q_ref.shape[0]
    quarter = (place[0] + rel(step)) % (tok_rows // rows)
    blocks = rows // WINDOW
    pairs = q_ref.shape[1] // LANES
    row = lax.broadcasted_iota(jnp.int32, (2 * WINDOW, WINDOW), 0) % WINDOW
    col = lax.broadcasted_iota(jnp.int32, (2 * WINDOW, WINDOW), 1)
    low = lax.broadcasted_iota(jnp.int32, (WINDOW, LANES), 1) < HEAD_DIM
    upper = lax.broadcasted_iota(jnp.int32, (2 * WINDOW, 1), 0) < WINDOW
    ones = jnp.ones((3 * WINDOW, LANES), jnp.bfloat16)
    finished = []
    for block in range(blocks):
        index = quarter * blocks + block
        at_start = jnp.where((place[1] == 0) & (index == 0), 4 * WINDOW, 0)
        at_end = jnp.where((place[1] == n_sp - 1) & (index == tok_rows // WINDOW - 1), 4 * WINDOW, 0)
        before_ok = col - row >= at_start
        after_ok = row - col >= at_end
        start = pl.multiple_of(index * WINDOW, WINDOW)
        mixed = []
        for pair in range(pairs):
            tile, half = (pair // 2, pair % 2)
            lanes = slice(tile * LANES, (tile + 1) * LANES)
            query = q_ref[block * WINDOW : (block + 1) * WINDOW, pair * LANES : (pair + 1) * LANES]
            query = query.astype(jnp.float32) * HEAD_DIM**-0.5
            turned = pltpu.roll(query, HEAD_DIM, 1)
            if half == 0:
                both = (jnp.where(low, query, 0.0), jnp.where(low, turned, 0.0))
            else:
                both = (jnp.where(low, 0.0, turned), jnp.where(low, 0.0, query))
            query = jnp.concatenate(both, axis=0).astype(jnp.bfloat16)
            keys = kv_ref[0, pl.ds(start, 3 * WINDOW), lanes]
            values = kv_ref[1, pl.ds(start, 3 * WINDOW), lanes]
            scores = lax.dot_general(
                query, keys, (((1,), (1,)), ((), ())), preferred_element_type=jnp.float32
            )
            before = jnp.where(before_ok, scores[:, :WINDOW], NEG)
            middle = scores[:, WINDOW : 2 * WINDOW]
            after = jnp.where(after_ok, scores[:, 2 * WINDOW :], NEG)
            sink_col = jnp.where(upper, sink[2 * pair], sink[2 * pair + 1])
            top = jnp.max(
                jnp.maximum(jnp.maximum(before, after), middle), axis=-1, keepdims=True
            )
            top = jnp.maximum(top, sink_col)
            expd = jnp.concatenate(
                [jnp.exp(part - top).astype(jnp.bfloat16) for part in (before, middle, after)],
                axis=1,
            )
            summed = jnp.dot(
                expd,
                jnp.concatenate([values, ones], axis=1),
                preferred_element_type=jnp.float32,
            )
            result = summed[:, :LANES] / (summed[:, LANES:] + jnp.exp(sink_col - top))
            first, second = (result[:WINDOW], result[WINDOW:])
            if half == 0:
                second = pltpu.roll(second, HEAD_DIM, 1)
            else:
                first = pltpu.roll(first, HEAD_DIM, 1)
            mixed.append(jnp.where(low, first, second).astype(jnp.bfloat16))
        finished.append(jnp.concatenate(mixed, axis=1))
    attended = jnp.concatenate(finished, axis=0)
    projected = jnp.dot(attended, w_ref[...], preferred_element_type=jnp.float32).astype(
        jnp.bfloat16
    )
    half = rows // 2
    for turn in range(len(out_refs) // 2):

        @pl.when(step == turn)
        def _():
            out_refs[2 * turn][...] = projected[:half]
            out_refs[2 * turn + 1][...] = projected[half:]


def attend(place, sink, queries, before, middle, after, out_weight, steps, rel, n_tp, n_sp):
    tok_rows, width = queries.shape
    rows = tok_rows // n_tp
    cols = out_weight.shape[1]

    def whole(array):
        return pl.BlockSpec(array.shape, lambda i, place, sink: (0,) * array.ndim)

    return pl.pallas_call(
        functools.partial(attend_kernel, rel=rel, n_sp=n_sp, tok_rows=tok_rows),
        grid_spec=pltpu.PrefetchScalarGridSpec(
            num_scalar_prefetch=2,
            grid=(steps,),
            in_specs=[
                pl.BlockSpec((rows, width), lambda i, place, sink: ((place[0] + rel(i)) % n_tp, 0)),
                whole(before),
                whole(middle),
                whole(after),
                whole(out_weight),
            ],
            out_specs=[pl.BlockSpec((rows // 2, cols), lambda i, place, sink: (0, 0))] * (2 * steps),
            scratch_shapes=[
                pltpu.VMEM((2, tok_rows + 2 * WINDOW, middle.shape[2]), jnp.bfloat16)
            ],
        ),
        out_shape=[jax.ShapeDtypeStruct((rows // 2, cols), jnp.bfloat16)] * (2 * steps),
        name="attend",
    )(place, sink, queries, before, middle, after, out_weight)


def normed(refs, gain, bias):
    values = refs[0][...].astype(jnp.float32)
    for ref in refs[1:]:
        values = values + ref[...].astype(jnp.float32)
    width = values.shape[1]
    mean = jnp.sum(values, axis=-1, keepdims=True) * (1.0 / width)
    centred = values - mean
    variance = jnp.sum(centred * centred, axis=-1, keepdims=True) * (1.0 / width)
    return (centred * lax.rsqrt(variance + 1e-06) * gain[...] + bias[...]).astype(jnp.bfloat16)


def norm_kernel(*refs):
    refs[-1][...] = normed(refs[:-3], *refs[-3:-1])


def norm_half(residual, side, parts, gain, bias, block=64):
    rows, width = parts[0].shape
    steps = rows // block
    tile = pl.BlockSpec((block, width), lambda i: (i, 0))
    line = pl.BlockSpec((1, width), lambda i: (0, 0))
    return pl.pallas_call(
        norm_kernel,
        grid=(steps,),
        in_specs=[pl.BlockSpec((block, width), lambda i: (side * steps + i, 0))]
        + [tile] * len(parts)
        + [line, line],
        out_specs=tile,
        out_shape=jax.ShapeDtypeStruct((rows, width), jnp.bfloat16),
        name="norm",
    )(residual, *parts, gain[None], bias[None])


def norm_both_kernel(*refs):
    *halves, gain, bias, out_ref = refs
    for side in range(2):

        @pl.when(pl.program_id(0) == side)
        def _():
            out_ref[...] = normed(halves[side::2], gain, bias)


def norm_both(halves, gain, bias):
    rows, width = halves[0].shape
    whole = pl.BlockSpec((rows, width), lambda i: (0, 0))
    line = pl.BlockSpec((1, width), lambda i: (0, 0))
    return pl.pallas_call(
        norm_both_kernel,
        grid=(2,),
        in_specs=[whole] * len(halves) + [line, line],
        out_specs=pl.BlockSpec((rows, width), lambda i: (i, 0)),
        out_shape=jax.ShapeDtypeStruct((2 * rows, width), jnp.bfloat16),
        name="norm_both",
    )(*halves, gain[None], bias[None])


def added(part, arrived):
    return (part.astype(jnp.float32) + arrived.astype(jnp.float32)).astype(jnp.bfloat16)


def feed_kernel(*refs, count):
    rows, (up_ref, down_ref), outs, acc = (
        refs[:count],
        refs[count : count + 2],
        refs[count + 2 : -1],
        refs[-1],
    )
    step = pl.program_id(0)
    width, block = (down_ref.shape[0] * down_ref.shape[2], up_ref.shape[3])
    tokens = jnp.concatenate([ref[...] for ref in rows], axis=0)
    hidden = jnp.dot(tokens, up_ref[...].reshape(-1, block), preferred_element_type=jnp.float32)
    activation = jnp.square(jnp.maximum(hidden, 0.0)).astype(jnp.bfloat16)
    branch = lax.dot_general(
        activation,
        down_ref[...].reshape(width, block),
        (((1,), (1,)), ((), ())),
        preferred_element_type=jnp.float32,
    )

    @pl.when(step == 0)
    def _():
        acc[...] = branch

    @pl.when((step > 0) & (step < pl.num_programs(0) - 1))
    def _():
        acc[...] += branch

    @pl.when(step == pl.num_programs(0) - 1)
    def _():
        total = (acc[...] + branch).astype(jnp.bfloat16)
        size = rows[0].shape[0]
        for index, out in enumerate(outs):
            out[...] = total[index * size : (index + 1) * size]


def feed_forward(rows, weights, block=512):
    size, width = rows[0].shape
    pieces, _, height, units = weights.shape
    whole = pl.BlockSpec((size, width), lambda i: (0, 0))
    return pl.pallas_call(
        functools.partial(feed_kernel, count=len(rows)),
        grid=(units // block,),
        in_specs=[whole] * len(rows)
        + [
            pl.BlockSpec((pieces, 1, height, block), lambda i: (0, 0, 0, i)),
            pl.BlockSpec((pieces, 1, height, block), lambda i: (0, 1, 0, i)),
        ],
        out_specs=[whole] * len(rows),
        out_shape=[jax.ShapeDtypeStruct((size, width), jnp.bfloat16)] * len(rows),
        scratch_shapes=[pltpu.VMEM((size * len(rows), width), jnp.float32)],
        compiler_params=pltpu.CompilerParams(vmem_limit_bytes=48 * 1024 * 1024),
        name="feed",
    )(*rows, weights, weights)


def on_device(
    residual_in,
    queries,
    keys_values,
    sink_logit,
    out_weight,
    norm1_gain,
    norm1_bias,
    up_weight,
    down_weight,
    norm2_gain,
    norm2_bias,
):
    n_tp, n_sp = (lax.axis_size("tp"), lax.axis_size("sp"))
    before, after = halo(keys_values, "sp", WINDOW)
    shards = jnp.concatenate([up_weight, down_weight.T], axis=0)
    weights = lax.all_gather(shards, "sp", axis=0, tiled=True).reshape(
        n_sp, 2, up_weight.shape[0], up_weight.shape[1]
    )
    place = jnp.where(
        jnp.arange(2, dtype=jnp.int32) == 0, lax.axis_index("tp"), lax.axis_index("sp")
    )
    run = functools.partial(
        attend, place, sink_logit, queries, before, keys_values, after, out_weight
    )
    far_top, far_bottom = run(1, lambda i: 2, n_tp, n_sp)
    from_left = shift(far_top, "tp", 1)
    from_right = shift(far_bottom, "tp", -1)
    right_top, right_bottom, left_top, left_bottom = run(2, lambda i: 1 + 2 * i, n_tp, n_sp)
    left_plain = shift(right_bottom, "tp", 1)
    right_plain = shift(left_top, "tp", -1)
    own_top, own_bottom = run(1, lambda i: 0, n_tp, n_sp)
    left_sum = shift(added(right_top, from_left), "tp", 1)
    right_sum = shift(added(left_bottom, from_right), "tp", -1)
    norm1 = (norm1_gain, norm1_bias)
    first_top = norm_half(residual_in, 0, (own_top, left_sum, right_plain), *norm1)
    first_bottom = norm_half(residual_in, 1, (own_bottom, left_plain, right_sum), *norm1)

    row_lt = shift(first_top, "tp", 1)
    row_rb = shift(first_bottom, "tp", -1)
    row_lb = shift(first_bottom, "tp", 1)
    row_rt = shift(first_top, "tp", -1)
    row_ft = shift(row_lt, "tp", 1)
    row_fb = shift(row_rb, "tp", -1)
    left_top, left_bottom, right_top, right_bottom = feed_forward(
        (row_lt, row_lb, row_rt, row_rb), weights
    )
    left_plain = shift(right_bottom, "tp", 1)
    right_plain = shift(left_top, "tp", -1)
    far_top, far_bottom = feed_forward((row_ft, row_fb), weights)
    from_left = shift(far_top, "tp", 1)
    from_right = shift(far_bottom, "tp", -1)
    own_top, own_bottom = feed_forward((first_top, first_bottom), weights)
    left_sum = shift(added(right_top, from_left), "tp", 1)
    right_sum = shift(added(left_bottom, from_right), "tp", -1)
    return norm_both(
        (first_top, first_bottom, own_top, own_bottom, left_sum, left_plain, right_plain, right_sum),
        norm2_gain,
        norm2_bias,
    )


def solution(mesh):
    return jax.shard_map(
        on_device,
        mesh=mesh,
        in_specs=(
            P(("sp", "tp"), None),
            P("sp", "tp"),
            P(None, "sp", "tp"),
            P("tp"),
            P("tp", None),
            P(),
            P(),
            P("sp", "tp"),
            P("tp", "sp"),
            P(),
            P(),
        ),
        out_specs=P(("sp", "tp"), None),
        check_vma=False,
    )
```

```python
import functools

import jax
import jax.numpy as jnp
from jax import lax
from jax.experimental import pallas as pl
from jax.experimental.pallas import tpu as pltpu
from jax.sharding import PartitionSpec as P


HEAD_DIM = 64
WINDOW = 128
LANES = 128
NEG = -1e30


def shift(value, step, axis="tp"):
    devices = lax.axis_size(axis)
    return lax.ppermute(value, axis, [(i, (i + step) % devices) for i in range(devices)])


def halo(shard, axis, width):
    devices, length = (lax.axis_size(axis), shard.shape[1])
    up = [(i, i + 1) for i in range(devices - 1)]
    down = [(j, i) for i, j in up]
    before = lax.ppermute(shard[:, length - width :], axis, up)
    after = lax.ppermute(shard[:, :width], axis, down)
    return before, after


def attend_kernel(
    place, sink, q_ref, before_ref, mid_ref, after_ref, w_ref, *refs, rel, n_sp, tok_rows
):
    *out_refs, kv_ref = refs
    step = pl.program_id(0)

    @pl.when(step == 0)
    def _():
        kv_ref[:, :WINDOW] = before_ref[...]
        kv_ref[:, WINDOW : WINDOW + tok_rows] = mid_ref[...]
        kv_ref[:, WINDOW + tok_rows :] = after_ref[...]

    rows = q_ref.shape[0]
    quarter = (place[0] + rel(step)) % (tok_rows // rows)
    blocks = rows // WINDOW
    pairs = q_ref.shape[1] // LANES
    row = lax.broadcasted_iota(jnp.int32, (2 * WINDOW, WINDOW), 0) % WINDOW
    col = lax.broadcasted_iota(jnp.int32, (2 * WINDOW, WINDOW), 1)
    low = lax.broadcasted_iota(jnp.int32, (WINDOW, LANES), 1) < HEAD_DIM
    upper = lax.broadcasted_iota(jnp.int32, (2 * WINDOW, 1), 0) < WINDOW
    ones = jnp.ones((3 * WINDOW, LANES), jnp.bfloat16)
    finished = []
    for block in range(blocks):
        index = quarter * blocks + block
        at_start = jnp.where((place[1] == 0) & (index == 0), 4 * WINDOW, 0)
        at_end = jnp.where((place[1] == n_sp - 1) & (index == tok_rows // WINDOW - 1), 4 * WINDOW, 0)
        before_ok = col - row >= at_start
        after_ok = row - col >= at_end
        start = pl.multiple_of(index * WINDOW, WINDOW)
        mixed = []
        for pair in range(pairs):
            tile, half = (pair // 2, pair % 2)
            lanes = slice(tile * LANES, (tile + 1) * LANES)
            query = q_ref[block * WINDOW : (block + 1) * WINDOW, pair * LANES : (pair + 1) * LANES]
            query = query.astype(jnp.float32) * HEAD_DIM**-0.5
            turned = pltpu.roll(query, HEAD_DIM, 1)
            if half == 0:
                both = (jnp.where(low, query, 0.0), jnp.where(low, turned, 0.0))
            else:
                both = (jnp.where(low, 0.0, turned), jnp.where(low, 0.0, query))
            query = jnp.concatenate(both, axis=0).astype(jnp.bfloat16)
            keys = kv_ref[0, pl.ds(start, 3 * WINDOW), lanes]
            values = kv_ref[1, pl.ds(start, 3 * WINDOW), lanes]
            scores = lax.dot_general(
                query, keys, (((1,), (1,)), ((), ())), preferred_element_type=jnp.float32
            )
            before = jnp.where(before_ok, scores[:, :WINDOW], NEG)
            middle = scores[:, WINDOW : 2 * WINDOW]
            after = jnp.where(after_ok, scores[:, 2 * WINDOW :], NEG)
            sink_col = jnp.where(upper, sink[2 * pair], sink[2 * pair + 1])
            top = jnp.max(
                jnp.maximum(jnp.maximum(before, after), middle), axis=-1, keepdims=True
            )
            top = jnp.maximum(top, sink_col)
            expd = jnp.concatenate(
                [jnp.exp(part - top).astype(jnp.bfloat16) for part in (before, middle, after)],
                axis=1,
            )
            summed = jnp.dot(
                expd,
                jnp.concatenate([values, ones], axis=1),
                preferred_element_type=jnp.float32,
            )
            result = summed[:, :LANES] / (summed[:, LANES:] + jnp.exp(sink_col - top))
            first, second = (result[:WINDOW], result[WINDOW:])
            if half == 0:
                second = pltpu.roll(second, HEAD_DIM, 1)
            else:
                first = pltpu.roll(first, HEAD_DIM, 1)
            mixed.append(jnp.where(low, first, second).astype(jnp.bfloat16))
        finished.append(jnp.concatenate(mixed, axis=1))
    attended = jnp.concatenate(finished, axis=0)
    projected = jnp.dot(attended, w_ref[...], preferred_element_type=jnp.float32).astype(
        jnp.bfloat16
    )
    half = rows // 2
    for turn in range(len(out_refs) // 2):

        @pl.when(step == turn)
        def _():
            out_refs[2 * turn][...] = projected[:half]
            out_refs[2 * turn + 1][...] = projected[half:]


def attend(place, sink, queries, before, middle, after, out_weight, steps, rel, n_tp, n_sp):
    tok_rows, width = queries.shape
    rows = tok_rows // n_tp
    cols = out_weight.shape[1]

    def whole(array):
        return pl.BlockSpec(array.shape, lambda i, place, sink: (0,) * array.ndim)

    return pl.pallas_call(
        functools.partial(attend_kernel, rel=rel, n_sp=n_sp, tok_rows=tok_rows),
        grid_spec=pltpu.PrefetchScalarGridSpec(
            num_scalar_prefetch=2,
            grid=(steps,),
            in_specs=[
                pl.BlockSpec((rows, width), lambda i, place, sink: ((place[0] + rel(i)) % n_tp, 0)),
                whole(before),
                whole(middle),
                whole(after),
                whole(out_weight),
            ],
            out_specs=[pl.BlockSpec((rows // 2, cols), lambda i, place, sink: (0, 0))] * (2 * steps),
            scratch_shapes=[
                pltpu.VMEM((2, tok_rows + 2 * WINDOW, middle.shape[2]), jnp.bfloat16)
            ],
        ),
        out_shape=[jax.ShapeDtypeStruct((rows // 2, cols), jnp.bfloat16)] * (2 * steps),
        name="attend",
    )(place, sink, queries, before, middle, after, out_weight)


def normed(refs, gain, bias):
    values = refs[0][...].astype(jnp.float32)
    for ref in refs[1:]:
        values = values + ref[...].astype(jnp.float32)
    width = values.shape[1]
    mean = jnp.sum(values, axis=-1, keepdims=True) * (1.0 / width)
    centred = values - mean
    variance = jnp.sum(centred * centred, axis=-1, keepdims=True) * (1.0 / width)
    return (centred * lax.rsqrt(variance + 1e-06) * gain[...] + bias[...]).astype(jnp.bfloat16)


def norm_kernel(*refs):
    refs[-1][...] = normed(refs[:-3], *refs[-3:-1])


def norm_half(residual, side, parts, gain, bias, block=64):
    rows, width = parts[0].shape
    steps = rows // block
    tile = pl.BlockSpec((block, width), lambda i: (i, 0))
    line = pl.BlockSpec((1, width), lambda i: (0, 0))
    return pl.pallas_call(
        norm_kernel,
        grid=(steps,),
        in_specs=[pl.BlockSpec((block, width), lambda i: (side * steps + i, 0))]
        + [tile] * len(parts)
        + [line, line],
        out_specs=tile,
        out_shape=jax.ShapeDtypeStruct((rows, width), jnp.bfloat16),
        name="norm",
    )(residual, *parts, gain[None], bias[None])


def norm_both_kernel(*refs):
    *halves, gain, bias, out_ref = refs
    for side in range(2):

        @pl.when(pl.program_id(0) == side)
        def _():
            out_ref[...] = normed(halves[side::2], gain, bias)


def norm_both(halves, gain, bias):
    rows, width = halves[0].shape
    whole = pl.BlockSpec((rows, width), lambda i: (0, 0))
    line = pl.BlockSpec((1, width), lambda i: (0, 0))
    return pl.pallas_call(
        norm_both_kernel,
        grid=(2,),
        in_specs=[whole] * len(halves) + [line, line],
        out_specs=pl.BlockSpec((rows, width), lambda i: (i, 0)),
        out_shape=jax.ShapeDtypeStruct((2 * rows, width), jnp.bfloat16),
        name="norm_both",
    )(*halves, gain[None], bias[None])


def added(part, arrived):
    return (part.astype(jnp.float32) + arrived.astype(jnp.float32)).astype(jnp.bfloat16)


def feed_kernel(*refs, count, chunk):
    rows, weights, outs = (refs[:count], refs[count], refs[count + 1 : 2 * count + 1])
    up, down, activation, sems = refs[2 * count + 1 :]
    pieces, height, units = up.shape
    size, steps = (rows[0].shape[0], units // chunk)
    part = pieces // steps
    width = part * height

    def up_copy(k):
        cols = pl.ds(pl.multiple_of(k * chunk, chunk), chunk)
        return pltpu.make_async_copy(weights.at[:, 0, :, cols], up.at[:, :, cols], sems.at[k])

    def down_copy(k):
        span = pl.ds(k * part, part)
        return pltpu.make_async_copy(weights.at[span, 1], down.at[span], sems.at[steps + k])

    for k in range(steps):
        up_copy(k).start()
    for k in range(steps):
        down_copy(k).start()

    @pl.loop(0, steps)
    def _(k):
        up_copy(k).wait()
        cols = pl.ds(pl.multiple_of(k * chunk, chunk), chunk)
        hidden = jnp.dot(
            jnp.concatenate([ref[...] for ref in rows], axis=0),
            up[:, :, cols].reshape(pieces * height, chunk),
            preferred_element_type=jnp.float32,
        )
        activation[:, cols] = jnp.square(jnp.maximum(hidden, 0.0)).astype(jnp.bfloat16)

    @pl.loop(0, steps)
    def _(k):
        down_copy(k).wait()
        branch = lax.dot_general(
            activation[...],
            down[pl.ds(k * part, part)].reshape(width, units),
            (((1,), (1,)), ((), ())),
            preferred_element_type=jnp.float32,
        ).astype(jnp.bfloat16)
        cols = pl.ds(pl.multiple_of(k * width, width), width)
        for index, out in enumerate(outs):
            out[:, cols] = branch[index * size : (index + 1) * size]


def feed_forward(rows, weights, chunk=512):
    size, width = rows[0].shape
    pieces, _, height, units = weights.shape
    whole = pl.BlockSpec(memory_space=pltpu.VMEM)
    full = pltpu.VMEM((pieces, height, units), jnp.bfloat16)
    return pl.pallas_call(
        functools.partial(feed_kernel, count=len(rows), chunk=chunk),
        in_specs=[whole] * len(rows) + [pl.BlockSpec(memory_space=pl.ANY)],
        out_specs=[whole] * len(rows),
        out_shape=[jax.ShapeDtypeStruct((size, width), jnp.bfloat16)] * len(rows),
        scratch_shapes=[
            full,
            full,
            pltpu.VMEM((size * len(rows), units), jnp.bfloat16),
            pltpu.SemaphoreType.DMA((2 * (units // chunk),)),
        ],
        compiler_params=pltpu.CompilerParams(vmem_limit_bytes=54 * 1024 * 1024),
        name="feed",
    )(*rows, weights)


def layer(
    residual_in,
    queries,
    keys_values,
    sink_logit,
    out_weight,
    norm1_gain,
    norm1_bias,
    up_weight,
    down_weight,
    norm2_gain,
    norm2_bias,
):
    n_tp, n_sp = (lax.axis_size("tp"), lax.axis_size("sp"))
    before, after = halo(keys_values, "sp", WINDOW)
    shards = jnp.concatenate([up_weight, down_weight.T], axis=0)
    weights = lax.all_gather(shards, "sp", axis=0, tiled=True).reshape(
        n_sp, 2, up_weight.shape[0], up_weight.shape[1]
    )
    place = jnp.where(
        jnp.arange(2, dtype=jnp.int32) == 0, lax.axis_index("tp"), lax.axis_index("sp")
    )
    run = functools.partial(
        attend, place, sink_logit, queries, before, keys_values, after, out_weight
    )
    far_top, far_bottom = run(1, lambda i: 2, n_tp, n_sp)
    from_left = shift(far_top, 1)
    from_right = shift(far_bottom, -1)
    right_top, right_bottom, left_top, left_bottom = run(2, lambda i: 1 + 2 * i, n_tp, n_sp)
    left_plain = shift(right_bottom, 1)
    right_plain = shift(left_top, -1)
    own_top, own_bottom = run(1, lambda i: 0, n_tp, n_sp)
    left_sum = shift(added(right_top, from_left), 1)
    right_sum = shift(added(left_bottom, from_right), -1)
    norm1 = (norm1_gain, norm1_bias)
    first_top = norm_half(residual_in, 0, (own_top, left_sum, right_plain), *norm1)
    first_bottom = norm_half(residual_in, 1, (own_bottom, left_plain, right_sum), *norm1)

    row_lt = shift(first_top, 1)
    row_rb = shift(first_bottom, -1)
    row_lb = shift(first_bottom, 1)
    row_rt = shift(first_top, -1)
    row_ft = shift(row_lt, 1)
    row_fb = shift(row_rb, -1)
    left_top, left_bottom, right_top, right_bottom = feed_forward(
        (row_lt, row_lb, row_rt, row_rb), weights
    )
    left_plain = shift(right_bottom, 1)
    right_plain = shift(left_top, -1)
    far_top, far_bottom = feed_forward((row_ft, row_fb), weights)
    from_left = shift(far_top, 1)
    from_right = shift(far_bottom, -1)
    own_top, own_bottom = feed_forward((first_top, first_bottom), weights)
    left_sum = shift(added(right_top, from_left), 1)
    right_sum = shift(added(left_bottom, from_right), -1)
    return norm_both(
        (first_top, first_bottom, own_top, own_bottom, left_sum, left_plain, right_plain, right_sum),
        norm2_gain,
        norm2_bias,
    )


def solution(mesh):
    return jax.shard_map(
        layer,
        mesh=mesh,
        in_specs=(
            P(("sp", "tp"), None),
            P("sp", "tp"),
            P(None, "sp", "tp"),
            P("tp"),
            P("tp", None),
            P(),
            P(),
            P("sp", "tp"),
            P("tp", "sp"),
            P(),
            P(),
        ),
        out_specs=P(("sp", "tp"), None),
        check_vma=False,
    )
```

```python
import functools

import jax
import jax.numpy as jnp
from jax import lax
from jax.experimental import pallas as pl
from jax.experimental.pallas import tpu as pltpu
from jax.sharding import PartitionSpec as P


HEAD_DIM = 64
WINDOW = 128
LANES = 128
NEG = -1e30


def shift(value, step, axis="tp"):
    devices = lax.axis_size(axis)
    return lax.ppermute(value, axis, [(i, (i + step) % devices) for i in range(devices)])


def halo(shard, axis, width):
    devices, length = (lax.axis_size(axis), shard.shape[1])
    up = [(i, i + 1) for i in range(devices - 1)]
    down = [(j, i) for i, j in up]
    before = lax.ppermute(shard[:, length - width :], axis, up)
    after = lax.ppermute(shard[:, :width], axis, down)
    return before, after


def attend_kernel(
    place, sink, q_ref, before_ref, mid_ref, after_ref, w_ref, *refs, rel, n_sp, tok_rows
):
    *out_refs, kv_ref = refs
    step = pl.program_id(0)

    @pl.when(step == 0)
    def _():
        kv_ref[:, :WINDOW] = before_ref[...]
        kv_ref[:, WINDOW : WINDOW + tok_rows] = mid_ref[...]
        kv_ref[:, WINDOW + tok_rows :] = after_ref[...]

    rows = q_ref.shape[0]
    quarter = (place[0] + rel(step)) % (tok_rows // rows)
    blocks = rows // WINDOW
    pairs = q_ref.shape[1] // LANES
    row = lax.broadcasted_iota(jnp.int32, (2 * WINDOW, WINDOW), 0) % WINDOW
    col = lax.broadcasted_iota(jnp.int32, (2 * WINDOW, WINDOW), 1)
    low = lax.broadcasted_iota(jnp.int32, (WINDOW, LANES), 1) < HEAD_DIM
    upper = lax.broadcasted_iota(jnp.int32, (2 * WINDOW, 1), 0) < WINDOW
    ones = jnp.ones((3 * WINDOW, LANES), jnp.bfloat16)
    finished = []
    for block in range(blocks):
        index = quarter * blocks + block
        at_start = jnp.where((place[1] == 0) & (index == 0), 4 * WINDOW, 0)
        at_end = jnp.where((place[1] == n_sp - 1) & (index == tok_rows // WINDOW - 1), 4 * WINDOW, 0)
        before_ok = col - row >= at_start
        after_ok = row - col >= at_end
        start = pl.multiple_of(index * WINDOW, WINDOW)
        mixed = []
        for pair in range(pairs):
            tile, half = (pair // 2, pair % 2)
            lanes = slice(tile * LANES, (tile + 1) * LANES)
            query = q_ref[block * WINDOW : (block + 1) * WINDOW, pair * LANES : (pair + 1) * LANES]
            query = query.astype(jnp.float32) * HEAD_DIM**-0.5
            turned = pltpu.roll(query, HEAD_DIM, 1)
            if half == 0:
                both = (jnp.where(low, query, 0.0), jnp.where(low, turned, 0.0))
            else:
                both = (jnp.where(low, 0.0, turned), jnp.where(low, 0.0, query))
            query = jnp.concatenate(both, axis=0).astype(jnp.bfloat16)
            keys = kv_ref[0, pl.ds(start, 3 * WINDOW), lanes]
            values = kv_ref[1, pl.ds(start, 3 * WINDOW), lanes]
            scores = lax.dot_general(
                query, keys, (((1,), (1,)), ((), ())), preferred_element_type=jnp.float32
            )
            before = jnp.where(before_ok, scores[:, :WINDOW], NEG)
            middle = scores[:, WINDOW : 2 * WINDOW]
            after = jnp.where(after_ok, scores[:, 2 * WINDOW :], NEG)
            sink_col = jnp.where(upper, sink[2 * pair], sink[2 * pair + 1])
            top = jnp.max(
                jnp.maximum(jnp.maximum(before, after), middle), axis=-1, keepdims=True
            )
            top = jnp.maximum(top, sink_col)
            expd = jnp.concatenate(
                [jnp.exp(part - top).astype(jnp.bfloat16) for part in (before, middle, after)],
                axis=1,
            )
            summed = jnp.dot(
                expd,
                jnp.concatenate([values, ones], axis=1),
                preferred_element_type=jnp.float32,
            )
            result = summed[:, :LANES] / (summed[:, LANES:] + jnp.exp(sink_col - top))
            first, second = (result[:WINDOW], result[WINDOW:])
            if half == 0:
                second = pltpu.roll(second, HEAD_DIM, 1)
            else:
                first = pltpu.roll(first, HEAD_DIM, 1)
            mixed.append(jnp.where(low, first, second).astype(jnp.bfloat16))
        finished.append(jnp.concatenate(mixed, axis=1))
    attended = jnp.concatenate(finished, axis=0)
    projected = jnp.dot(attended, w_ref[...], preferred_element_type=jnp.float32).astype(
        jnp.bfloat16
    )
    half = rows // 2
    for turn in range(len(out_refs) // 2):

        @pl.when(step == turn)
        def _():
            out_refs[2 * turn][...] = projected[:half]
            out_refs[2 * turn + 1][...] = projected[half:]


def attend(place, sink, queries, before, middle, after, out_weight, steps, rel, n_tp, n_sp):
    tok_rows, width = queries.shape
    rows = tok_rows // n_tp
    cols = out_weight.shape[1]

    def whole(array):
        return pl.BlockSpec(array.shape, lambda i, place, sink: (0,) * array.ndim)

    return pl.pallas_call(
        functools.partial(attend_kernel, rel=rel, n_sp=n_sp, tok_rows=tok_rows),
        grid_spec=pltpu.PrefetchScalarGridSpec(
            num_scalar_prefetch=2,
            grid=(steps,),
            in_specs=[
                pl.BlockSpec((rows, width), lambda i, place, sink: ((place[0] + rel(i)) % n_tp, 0)),
                whole(before),
                whole(middle),
                whole(after),
                whole(out_weight),
            ],
            out_specs=[pl.BlockSpec((rows // 2, cols), lambda i, place, sink: (0, 0))] * (2 * steps),
            scratch_shapes=[
                pltpu.VMEM((2, tok_rows + 2 * WINDOW, middle.shape[2]), jnp.bfloat16)
            ],
        ),
        out_shape=[jax.ShapeDtypeStruct((rows // 2, cols), jnp.bfloat16)] * (2 * steps),
        name="attend",
    )(place, sink, queries, before, middle, after, out_weight)


def normed(refs, gain, bias):
    values = refs[0][...].astype(jnp.float32)
    for ref in refs[1:]:
        values = values + ref[...].astype(jnp.float32)
    width = values.shape[1]
    mean = jnp.sum(values, axis=-1, keepdims=True) * (1.0 / width)
    centred = values - mean
    variance = jnp.sum(centred * centred, axis=-1, keepdims=True) * (1.0 / width)
    return (centred * lax.rsqrt(variance + 1e-06) * gain[...] + bias[...]).astype(jnp.bfloat16)


def norm_kernel(*refs, whole):
    *parts, gain, bias, out_ref = refs
    for side in range(2):

        @pl.when(pl.program_id(0) // (pl.num_programs(0) // 2) == side)
        def _():
            out_ref[...] = normed(parts[:whole] + parts[whole + side :: 2], gain, bias)


def norm_rows(wholes, halves, gain, bias, block=64):
    rows, width = wholes[0].shape
    steps = rows // block
    half = steps // 2
    tile = pl.BlockSpec((block, width), lambda i: (i, 0))
    tops = pl.BlockSpec((block, width), lambda i: (jnp.minimum(i, half - 1), 0))
    bottoms = pl.BlockSpec((block, width), lambda i: (jnp.maximum(i - half, 0), 0))
    line = pl.BlockSpec((1, width), lambda i: (0, 0))
    return pl.pallas_call(
        functools.partial(norm_kernel, whole=len(wholes)),
        grid=(steps,),
        in_specs=[tile] * len(wholes) + [tops, bottoms] * (len(halves) // 2) + [line, line],
        out_specs=tile,
        out_shape=jax.ShapeDtypeStruct((rows, width), jnp.bfloat16),
        name="norm",
    )(*wholes, *halves, gain[None], bias[None])


def added(part, arrived):
    return (part.astype(jnp.float32) + arrived.astype(jnp.float32)).astype(jnp.bfloat16)


def feed_kernel(*refs, count, outs, chunk):
    rows, weights, results = (refs[:count], refs[count], refs[count + 1 : count + 1 + outs])
    tokens, up, down, activation, branch, sems = refs[count + 1 + outs :]
    pieces, height, units = up.shape
    size, steps = (rows[0].shape[0], units // chunk)
    height_out = results[0].shape[0]
    part = pieces // steps
    width = part * height

    def row_copy(index):
        span = pl.ds(index * size, size)
        return pltpu.make_async_copy(rows[index], tokens.at[span], sems.at[2 * steps + index])

    def up_copy(k):
        cols = pl.ds(pl.multiple_of(k * chunk, chunk), chunk)
        return pltpu.make_async_copy(weights.at[:, 0, :, cols], up.at[:, :, cols], sems.at[k])

    def down_copy(k):
        span = pl.ds(k * part, part)
        return pltpu.make_async_copy(weights.at[span, 1], down.at[span], sems.at[steps + k])

    def out_copy(index, k):
        cols = pl.ds(pl.multiple_of(k * width, width), width)
        span = pl.ds(index * height_out, height_out)
        return pltpu.make_async_copy(
            branch.at[span, cols],
            results[index].at[:, cols],
            sems.at[2 * steps + count + index * steps + k],
        )

    for index in range(count):
        row_copy(index).start()
    for k in range(steps):
        up_copy(k).start()
    for k in range(steps):
        down_copy(k).start()
    for index in range(count):
        row_copy(index).wait()

    @pl.loop(0, steps)
    def _(k):
        up_copy(k).wait()
        cols = pl.ds(pl.multiple_of(k * chunk, chunk), chunk)
        hidden = jnp.dot(
            tokens[...],
            up[:, :, cols].reshape(pieces * height, chunk),
            preferred_element_type=jnp.float32,
        )
        activation[:, cols] = jnp.square(jnp.maximum(hidden, 0.0)).astype(jnp.bfloat16)

    @pl.loop(0, steps)
    def _(k):
        down_copy(k).wait()
        cols = pl.ds(pl.multiple_of(k * width, width), width)
        branch[:, cols] = lax.dot_general(
            activation[...],
            down[pl.ds(k * part, part)].reshape(width, units),
            (((1,), (1,)), ((), ())),
            preferred_element_type=jnp.float32,
        ).astype(jnp.bfloat16)
        for index in range(outs):
            out_copy(index, k).start()

    @pl.loop(0, steps)
    def _(k):
        for index in range(outs):
            out_copy(index, k).wait()


def feed_forward(rows, weights, height_out, chunk=512):
    size, width = rows[0].shape
    pieces, _, height, units = weights.shape
    count, total = (len(rows), len(rows) * size)
    outs = total // height_out
    anywhere = pl.BlockSpec(memory_space=pl.ANY)
    full = pltpu.VMEM((pieces, height, units), jnp.bfloat16)
    steps = units // chunk
    return pl.pallas_call(
        functools.partial(feed_kernel, count=count, outs=outs, chunk=chunk),
        in_specs=[anywhere] * (count + 1),
        out_specs=[anywhere] * outs,
        out_shape=[jax.ShapeDtypeStruct((height_out, width), jnp.bfloat16)] * outs,
        scratch_shapes=[
            pltpu.VMEM((total, width), jnp.bfloat16),
            full,
            full,
            pltpu.VMEM((total, units), jnp.bfloat16),
            pltpu.VMEM((total, width), jnp.bfloat16),
            pltpu.SemaphoreType.DMA((2 * steps + count + outs * steps,)),
        ],
        compiler_params=pltpu.CompilerParams(vmem_limit_bytes=40 * 1024 * 1024),
        name="feed",
    )(*rows, weights)


def layer(
    residual_in,
    queries,
    keys_values,
    sink_logit,
    out_weight,
    norm1_gain,
    norm1_bias,
    up_weight,
    down_weight,
    norm2_gain,
    norm2_bias,
):
    n_tp, n_sp = (lax.axis_size("tp"), lax.axis_size("sp"))
    before, after = halo(keys_values, "sp", WINDOW)
    shards = jnp.concatenate([up_weight, down_weight.T], axis=0)
    weights = lax.all_gather(shards, "sp", axis=0, tiled=True).reshape(
        n_sp, 2, up_weight.shape[0], up_weight.shape[1]
    )
    place = jnp.where(
        jnp.arange(2, dtype=jnp.int32) == 0, lax.axis_index("tp"), lax.axis_index("sp")
    )
    run = functools.partial(
        attend, place, sink_logit, queries, before, keys_values, after, out_weight
    )
    far_top, far_bottom = run(1, lambda i: 2, n_tp, n_sp)
    from_left = shift(far_top, 1)
    from_right = shift(far_bottom, -1)
    right_top, right_bottom, left_top, left_bottom = run(2, lambda i: 1 + 2 * i, n_tp, n_sp)
    left_plain = shift(right_bottom, 1)
    right_plain = shift(left_top, -1)
    own_top, own_bottom = run(1, lambda i: 0, n_tp, n_sp)
    left_sum = shift(added(right_top, from_left), 1)
    right_sum = shift(added(left_bottom, from_right), -1)
    first = norm_rows(
        (residual_in,),
        (own_top, own_bottom, left_sum, left_plain, right_plain, right_sum),
        norm1_gain,
        norm1_bias,
    )

    half = first.shape[0] // 2
    row_left = shift(first, 1)
    row_right = shift(first, -1)
    row_ft = shift(row_left[:half], 1)
    row_fb = shift(row_right[half:], -1)
    left_top, left_bottom, right_top, right_bottom = feed_forward(
        (row_left, row_right), weights, half
    )
    left_plain = shift(right_bottom, 1)
    right_plain = shift(left_top, -1)
    far_top, far_bottom = feed_forward((row_ft, row_fb), weights, half)
    from_left = shift(far_top, 1)
    from_right = shift(far_bottom, -1)
    (own,) = feed_forward((first,), weights, 2 * half)
    left_sum = shift(added(right_top, from_left), 1)
    right_sum = shift(added(left_bottom, from_right), -1)
    return norm_rows(
        (first, own), (left_sum, left_plain, right_plain, right_sum), norm2_gain, norm2_bias
    )


def solution(mesh):
    return jax.shard_map(
        layer,
        mesh=mesh,
        in_specs=(
            P(("sp", "tp"), None),
            P("sp", "tp"),
            P(None, "sp", "tp"),
            P("tp"),
            P("tp", None),
            P(),
            P(),
            P("sp", "tp"),
            P("tp", "sp"),
            P(),
            P(),
        ),
        out_specs=P(("sp", "tp"), None),
        check_vma=False,
    )
```

```python
import functools

import jax
import jax.numpy as jnp
from jax import lax
from jax.experimental import pallas as pl
from jax.experimental.pallas import tpu as pltpu
from jax.sharding import PartitionSpec as P


HEAD_DIM = 64
WINDOW = 128
LANES = 128
NEG = -1e30


def shift(value, step, axis="tp"):
    devices = lax.axis_size(axis)
    return lax.ppermute(value, axis, [(i, (i + step) % devices) for i in range(devices)])


def halo(shard, axis, width):
    devices, length = (lax.axis_size(axis), shard.shape[1])
    up = [(i, i + 1) for i in range(devices - 1)]
    down = [(j, i) for i, j in up]
    before = lax.ppermute(shard[:, length - width :], axis, up)
    after = lax.ppermute(shard[:, :width], axis, down)
    return before, after


def attend_kernel(
    place, sink, q_ref, before_ref, mid_ref, after_ref, w_ref, *refs, rel, n_sp, tok_rows
):
    *out_refs, kv_ref, weight_ref, sems = refs
    step = pl.program_id(0)
    kv_copies = [
        pltpu.make_async_copy(ref, kv_ref.at[:, pl.ds(at, ref.shape[1])], sems.at[index])
        for index, (ref, at) in enumerate(
            ((before_ref, 0), (mid_ref, WINDOW), (after_ref, WINDOW + tok_rows))
        )
    ]
    weight_copy = pltpu.make_async_copy(w_ref, weight_ref, sems.at[3])

    @pl.when(step == 0)
    def _():
        for copy in kv_copies:
            copy.start()
        weight_copy.start()
        for copy in kv_copies:
            copy.wait()

    rows = q_ref.shape[0]
    quarter = (place[0] + rel(step)) % (tok_rows // rows)
    blocks = rows // WINDOW
    pairs = q_ref.shape[1] // LANES
    row = lax.broadcasted_iota(jnp.int32, (2 * WINDOW, WINDOW), 0) % WINDOW
    col = lax.broadcasted_iota(jnp.int32, (2 * WINDOW, WINDOW), 1)
    low = lax.broadcasted_iota(jnp.int32, (WINDOW, LANES), 1) < HEAD_DIM
    upper = lax.broadcasted_iota(jnp.int32, (2 * WINDOW, 1), 0) < WINDOW
    ones = jnp.ones((3 * WINDOW, LANES), jnp.bfloat16)
    finished = []
    for block in range(blocks):
        index = quarter * blocks + block
        at_start = jnp.where((place[1] == 0) & (index == 0), 4 * WINDOW, 0)
        at_end = jnp.where((place[1] == n_sp - 1) & (index == tok_rows // WINDOW - 1), 4 * WINDOW, 0)
        before_ok = col - row >= at_start
        after_ok = row - col >= at_end
        start = pl.multiple_of(index * WINDOW, WINDOW)
        mixed = []
        for pair in range(pairs):
            tile, half = (pair // 2, pair % 2)
            lanes = slice(tile * LANES, (tile + 1) * LANES)
            query = q_ref[block * WINDOW : (block + 1) * WINDOW, pair * LANES : (pair + 1) * LANES]
            query = query.astype(jnp.float32) * HEAD_DIM**-0.5
            turned = pltpu.roll(query, HEAD_DIM, 1)
            if half == 0:
                both = (jnp.where(low, query, 0.0), jnp.where(low, turned, 0.0))
            else:
                both = (jnp.where(low, 0.0, turned), jnp.where(low, 0.0, query))
            query = jnp.concatenate(both, axis=0).astype(jnp.bfloat16)
            keys = kv_ref[0, pl.ds(start, 3 * WINDOW), lanes]
            values = kv_ref[1, pl.ds(start, 3 * WINDOW), lanes]
            scores = lax.dot_general(
                query, keys, (((1,), (1,)), ((), ())), preferred_element_type=jnp.float32
            )
            before = jnp.where(before_ok, scores[:, :WINDOW], NEG)
            middle = scores[:, WINDOW : 2 * WINDOW]
            after = jnp.where(after_ok, scores[:, 2 * WINDOW :], NEG)
            sink_col = jnp.where(upper, sink[2 * pair], sink[2 * pair + 1])
            top = jnp.max(
                jnp.maximum(jnp.maximum(before, after), middle), axis=-1, keepdims=True
            )
            top = jnp.maximum(top, sink_col)
            expd = jnp.concatenate(
                [jnp.exp(part - top).astype(jnp.bfloat16) for part in (before, middle, after)],
                axis=1,
            )
            summed = jnp.dot(
                expd,
                jnp.concatenate([values, ones], axis=1),
                preferred_element_type=jnp.float32,
            )
            result = summed[:, :LANES] / (summed[:, LANES:] + jnp.exp(sink_col - top))
            first, second = (result[:WINDOW], result[WINDOW:])
            if half == 0:
                second = pltpu.roll(second, HEAD_DIM, 1)
            else:
                first = pltpu.roll(first, HEAD_DIM, 1)
            mixed.append(jnp.where(low, first, second).astype(jnp.bfloat16))
        finished.append(jnp.concatenate(mixed, axis=1))
    attended = jnp.concatenate(finished, axis=0)

    @pl.when(step == 0)
    def _():
        weight_copy.wait()

    projected = jnp.dot(attended, weight_ref[...], preferred_element_type=jnp.float32).astype(
        jnp.bfloat16
    )
    half = rows // 2
    for turn in range(len(out_refs) // 2):

        @pl.when(step == turn)
        def _():
            out_refs[2 * turn][...] = projected[:half]
            out_refs[2 * turn + 1][...] = projected[half:]


def attend(place, sink, queries, before, middle, after, out_weight, steps, rel, n_tp, n_sp):
    tok_rows, width = queries.shape
    rows = tok_rows // n_tp
    cols = out_weight.shape[1]

    anywhere = pl.BlockSpec(memory_space=pl.ANY)
    return pl.pallas_call(
        functools.partial(attend_kernel, rel=rel, n_sp=n_sp, tok_rows=tok_rows),
        grid_spec=pltpu.PrefetchScalarGridSpec(
            num_scalar_prefetch=2,
            grid=(steps,),
            in_specs=[
                pl.BlockSpec((rows, width), lambda i, place, sink: ((place[0] + rel(i)) % n_tp, 0)),
                anywhere,
                anywhere,
                anywhere,
                anywhere,
            ],
            out_specs=[pl.BlockSpec((rows // 2, cols), lambda i, place, sink: (0, 0))] * (2 * steps),
            scratch_shapes=[
                pltpu.VMEM((2, tok_rows + 2 * WINDOW, middle.shape[2]), jnp.bfloat16),
                pltpu.VMEM(out_weight.shape, jnp.bfloat16),
                pltpu.SemaphoreType.DMA((4,)),
            ],
        ),
        out_shape=[jax.ShapeDtypeStruct((rows // 2, cols), jnp.bfloat16)] * (2 * steps),
        compiler_params=pltpu.CompilerParams(vmem_limit_bytes=24 * 1024 * 1024),
        name="attend",
    )(place, sink, queries, before, middle, after, out_weight)


def norm_kernel(*refs, tops, bottoms, outs, block):
    count = max(max(tops), max(bottoms)) + 1
    sources, (gain, bias), results = (refs[:count], refs[count : count + 2], refs[count + 2 : -3])
    parts, out, sems = refs[-3:]
    rows, width = out.shape
    steps = rows // block
    half = steps // 2

    def in_copy(step, place):
        ref = sources[(tops if step < half else bottoms)[place]]
        at = step * block % ref.shape[0]
        return pltpu.make_async_copy(
            ref.at[pl.ds(at, block)],
            parts.at[place, pl.ds(step * block, block)],
            sems.at[step * (len(tops) + 1) + place],
        )

    def out_copy(step):
        ref = results[step * block // (rows // outs)]
        at = step * block % ref.shape[0]
        return pltpu.make_async_copy(
            out.at[pl.ds(step * block, block)],
            ref.at[pl.ds(at, block)],
            sems.at[step * (len(tops) + 1) + len(tops)],
        )

    for step in range(steps):
        for place in range(len(tops)):
            in_copy(step, place).start()
    for step in range(steps):
        span = slice(step * block, (step + 1) * block)
        values = None
        for place in range(len(tops)):
            in_copy(step, place).wait()
        for place in range(len(tops)):
            part = parts[place, span].astype(jnp.float32)
            values = part if values is None else values + part
        mean = jnp.sum(values, axis=-1, keepdims=True) * (1.0 / width)
        centred = values - mean
        variance = jnp.sum(centred * centred, axis=-1, keepdims=True) * (1.0 / width)
        out[span] = (centred * lax.rsqrt(variance + 1e-06) * gain[...] + bias[...]).astype(
            jnp.bfloat16
        )
        out_copy(step).start()
    for step in range(steps):
        out_copy(step).wait()


def norm_rows(sources, tops, bottoms, outs, gain, bias, rows, block=64):
    width = sources[0].shape[1]
    anywhere = pl.BlockSpec(memory_space=pl.ANY)
    vmem = pl.BlockSpec(memory_space=pltpu.VMEM)
    steps = rows // block
    return pl.pallas_call(
        functools.partial(norm_kernel, tops=tops, bottoms=bottoms, outs=outs, block=block),
        in_specs=[anywhere] * len(sources) + [vmem, vmem],
        out_specs=[anywhere] * outs,
        out_shape=[jax.ShapeDtypeStruct((rows // outs, width), jnp.bfloat16)] * outs,
        scratch_shapes=[
            pltpu.VMEM((len(tops), rows, width), jnp.bfloat16),
            pltpu.VMEM((rows, width), jnp.bfloat16),
            pltpu.SemaphoreType.DMA((steps * (len(tops) + 1),)),
        ],
        compiler_params=pltpu.CompilerParams(vmem_limit_bytes=16 * 1024 * 1024),
        name="norm",
    )(*sources, gain[None], bias[None])


def added(part, arrived):
    return (part.astype(jnp.float32) + arrived.astype(jnp.float32)).astype(jnp.bfloat16)


def feed_kernel(*refs, count, outs, chunk):
    rows, weights, results = (refs[:count], refs[count], refs[count + 1 : count + 1 + outs])
    tokens, up, down, activation, branch, sems = refs[count + 1 + outs :]
    pieces, height, units = up.shape
    size, steps = (rows[0].shape[0], units // chunk)
    height_out = results[0].shape[0]
    part = pieces // steps
    width = part * height

    def row_copy(index):
        span = pl.ds(index * size, size)
        return pltpu.make_async_copy(rows[index], tokens.at[span], sems.at[2 * steps + index])

    def up_copy(k):
        cols = pl.ds(pl.multiple_of(k * chunk, chunk), chunk)
        return pltpu.make_async_copy(weights.at[:, 0, :, cols], up.at[:, :, cols], sems.at[k])

    def down_copy(k):
        span = pl.ds(k * part, part)
        return pltpu.make_async_copy(weights.at[span, 1], down.at[span], sems.at[steps + k])

    def out_copy(index, k):
        cols = pl.ds(pl.multiple_of(k * width, width), width)
        span = pl.ds(index * height_out, height_out)
        return pltpu.make_async_copy(
            branch.at[span, cols],
            results[index].at[:, cols],
            sems.at[2 * steps + count + index * steps + k],
        )

    for index in range(count):
        row_copy(index).start()
    for k in range(steps):
        up_copy(k).start()
    for k in range(steps):
        down_copy(k).start()
    for index in range(count):
        row_copy(index).wait()

    @pl.loop(0, steps)
    def _(k):
        up_copy(k).wait()
        cols = pl.ds(pl.multiple_of(k * chunk, chunk), chunk)
        hidden = jnp.dot(
            tokens[...],
            up[:, :, cols].reshape(pieces * height, chunk),
            preferred_element_type=jnp.float32,
        )
        activation[:, cols] = jnp.square(jnp.maximum(hidden, 0.0)).astype(jnp.bfloat16)

    @pl.loop(0, steps)
    def _(k):
        down_copy(k).wait()
        cols = pl.ds(pl.multiple_of(k * width, width), width)
        branch[:, cols] = lax.dot_general(
            activation[...],
            down[pl.ds(k * part, part)].reshape(width, units),
            (((1,), (1,)), ((), ())),
            preferred_element_type=jnp.float32,
        ).astype(jnp.bfloat16)
        for index in range(outs):
            out_copy(index, k).start()

    @pl.loop(0, steps)
    def _(k):
        for index in range(outs):
            out_copy(index, k).wait()


def feed_forward(rows, weights, height_out, chunk=512):
    size, width = rows[0].shape
    pieces, _, height, units = weights.shape
    count, total = (len(rows), len(rows) * size)
    outs = total // height_out
    anywhere = pl.BlockSpec(memory_space=pl.ANY)
    full = pltpu.VMEM((pieces, height, units), jnp.bfloat16)
    steps = units // chunk
    return pl.pallas_call(
        functools.partial(feed_kernel, count=count, outs=outs, chunk=chunk),
        in_specs=[anywhere] * (count + 1),
        out_specs=[anywhere] * outs,
        out_shape=[jax.ShapeDtypeStruct((height_out, width), jnp.bfloat16)] * outs,
        scratch_shapes=[
            pltpu.VMEM((total, width), jnp.bfloat16),
            full,
            full,
            pltpu.VMEM((total, units), jnp.bfloat16),
            pltpu.VMEM((total, width), jnp.bfloat16),
            pltpu.SemaphoreType.DMA((2 * steps + count + outs * steps,)),
        ],
        compiler_params=pltpu.CompilerParams(vmem_limit_bytes=40 * 1024 * 1024),
        name="feed",
    )(*rows, weights)


def layer(
    residual_in,
    queries,
    keys_values,
    sink_logit,
    out_weight,
    norm1_gain,
    norm1_bias,
    up_weight,
    down_weight,
    norm2_gain,
    norm2_bias,
):
    n_tp, n_sp = (lax.axis_size("tp"), lax.axis_size("sp"))
    before, after = halo(keys_values, "sp", WINDOW)
    shards = jnp.concatenate([up_weight, down_weight.T], axis=0)
    weights = lax.all_gather(shards, "sp", axis=0, tiled=True).reshape(
        n_sp, 2, up_weight.shape[0], up_weight.shape[1]
    )
    place = jnp.where(
        jnp.arange(2, dtype=jnp.int32) == 0, lax.axis_index("tp"), lax.axis_index("sp")
    )
    run = functools.partial(
        attend, place, sink_logit, queries, before, keys_values, after, out_weight
    )
    far_top, far_bottom = run(1, lambda i: 2, n_tp, n_sp)
    from_left = shift(far_top, 1)
    from_right = shift(far_bottom, -1)
    right_top, right_bottom, left_top, left_bottom = run(2, lambda i: 1 + 2 * i, n_tp, n_sp)
    left_plain = shift(right_bottom, 1)
    right_plain = shift(left_top, -1)
    own_top, own_bottom = run(1, lambda i: 0, n_tp, n_sp)
    left_sum = shift(added(right_top, from_left), 1)
    right_sum = shift(added(left_bottom, from_right), -1)
    rows, half = (2 * own_top.shape[0], own_top.shape[0])
    first_top, first_bottom = norm_rows(
        (residual_in, own_top, own_bottom, left_sum, left_plain, right_plain, right_sum),
        (0, 1, 3, 5),
        (0, 2, 4, 6),
        2,
        norm1_gain,
        norm1_bias,
        rows,
    )

    row_lt = shift(first_top, 1)
    row_rb = shift(first_bottom, -1)
    row_lb = shift(first_bottom, 1)
    row_rt = shift(first_top, -1)
    row_ft = shift(row_lt, 1)
    row_fb = shift(row_rb, -1)
    left_top, right_bottom = feed_forward((row_lt, row_rb), weights, half)
    left_plain = shift(right_bottom, 1)
    right_plain = shift(left_top, -1)
    far_top, far_bottom = feed_forward((row_ft, row_fb), weights, half)
    from_left = shift(far_top, 1)
    from_right = shift(far_bottom, -1)
    left_bottom, right_top = feed_forward((row_lb, row_rt), weights, half)
    left_sum = shift(added(right_top, from_left), 1)
    right_sum = shift(added(left_bottom, from_right), -1)
    own_top, own_bottom = feed_forward((first_top, first_bottom), weights, half)
    (out,) = norm_rows(
        (
            first_top,
            first_bottom,
            own_top,
            own_bottom,
            left_sum,
            left_plain,
            right_plain,
            right_sum,
        ),
        (0, 2, 4, 6),
        (1, 3, 5, 7),
        1,
        norm2_gain,
        norm2_bias,
        rows,
    )
    return out


def solution(mesh):
    return jax.shard_map(
        layer,
        mesh=mesh,
        in_specs=(
            P(("sp", "tp"), None),
            P("sp", "tp"),
            P(None, "sp", "tp"),
            P("tp"),
            P("tp", None),
            P(),
            P(),
            P("sp", "tp"),
            P("tp", "sp"),
            P(),
            P(),
        ),
        out_specs=P(("sp", "tp"), None),
        check_vma=False,
    )
```

```python
import functools

import jax
import jax.numpy as jnp
from jax import lax
from jax.experimental import pallas as pl
from jax.experimental.pallas import tpu as pltpu
from jax.sharding import PartitionSpec as P


HEAD_DIM = 64
WINDOW = 128
LANES = 128
NEG = -1e30


def shift(value, step, axis="tp"):
    devices = lax.axis_size(axis)
    return lax.ppermute(value, axis, [(i, (i + step) % devices) for i in range(devices)])


def prepare_kernel(up, down, keys_values, joined, last, first, sems):
    height, tok_rows = (up.shape[0], keys_values.shape[1])
    copies = [
        pltpu.make_async_copy(source, target, sems.at[index])
        for index, (source, target) in enumerate(
            (
                (keys_values.at[:, pl.ds(tok_rows - WINDOW, WINDOW)], last),
                (keys_values.at[:, pl.ds(0, WINDOW)], first),
                (up, joined.at[pl.ds(0, height)]),
                (down, joined.at[pl.ds(height, height)]),
            )
        )
    ]
    for copy in copies:
        copy.start()
    for copy in copies:
        copy.wait()


def prepare(up, down, keys_values):
    anywhere = pl.BlockSpec(memory_space=pl.ANY)
    edge = jax.ShapeDtypeStruct((2, WINDOW, keys_values.shape[2]), jnp.bfloat16)
    return pl.pallas_call(
        prepare_kernel,
        in_specs=[pl.BlockSpec(memory_space=pltpu.HBM)] * 3,
        out_specs=[pl.BlockSpec(memory_space=pltpu.HBM), anywhere, anywhere],
        out_shape=[
            jax.ShapeDtypeStruct((2 * up.shape[0], up.shape[1]), jnp.bfloat16),
            edge,
            edge,
        ],
        scratch_shapes=[pltpu.SemaphoreType.DMA((4,))],
        compiler_params=pltpu.CompilerParams(vmem_limit_bytes=60 * 1024 * 1024),
        name="prepare",
    )(up, down, keys_values)


def halo(last, first, axis):
    devices = lax.axis_size(axis)
    up = [(i, i + 1) for i in range(devices - 1)]
    down = [(j, i) for i, j in up]
    before = lax.ppermute(last, axis, up)
    after = lax.ppermute(first, axis, down)
    return before, after


def attend_kernel(sink, q_hbm, before_ref, mid_ref, after_ref, w_ref, *refs, rels):
    *out_refs, q_ref, kv_ref, weight_ref, sems = refs
    step = pl.program_id(0)
    rows, tok_rows = (q_ref.shape[1], mid_ref.shape[1])
    count = tok_rows // rows
    n_sp = lax.axis_size("sp")
    token_group, head_group = (lax.axis_index("sp"), lax.axis_index("tp"))
    rel = rels[-1]
    for turn in reversed(range(len(rels) - 1)):
        rel = jnp.where(step == turn, rels[turn], rel)
    quarter = (head_group + rel) % count
    copies = [
        pltpu.make_async_copy(ref, kv_ref.at[:, pl.ds(at, ref.shape[1])], sems.at[index])
        for index, (ref, at) in enumerate(
            ((before_ref, 0), (mid_ref, WINDOW), (after_ref, WINDOW + tok_rows))
        )
    ] + [
        pltpu.make_async_copy(
            q_hbm.at[pl.ds(pl.multiple_of((head_group + turn) % count * rows, rows), rows)],
            q_ref.at[index],
            sems.at[4 + index],
        )
        for index, turn in enumerate(rels)
    ]
    weight_copy = pltpu.make_async_copy(w_ref, weight_ref, sems.at[3])

    @pl.when(step == 0)
    def _():
        for copy in copies:
            copy.start()
        weight_copy.start()
        for copy in copies:
            copy.wait()

    blocks = rows // WINDOW
    pairs = q_ref.shape[2] // LANES
    row = lax.broadcasted_iota(jnp.int32, (2 * WINDOW, WINDOW), 0) % WINDOW
    col = lax.broadcasted_iota(jnp.int32, (2 * WINDOW, WINDOW), 1)
    low = lax.broadcasted_iota(jnp.int32, (WINDOW, LANES), 1) < HEAD_DIM
    upper = lax.broadcasted_iota(jnp.int32, (2 * WINDOW, 1), 0) < WINDOW
    ones = jnp.ones((3 * WINDOW, LANES), jnp.bfloat16)
    finished = []
    for block in range(blocks):
        index = quarter * blocks + block
        at_start = jnp.where((token_group == 0) & (index == 0), 4 * WINDOW, 0)
        at_end = jnp.where((token_group == n_sp - 1) & (index == tok_rows // WINDOW - 1), 4 * WINDOW, 0)
        before_ok = col - row >= at_start
        after_ok = row - col >= at_end
        start = pl.multiple_of(index * WINDOW, WINDOW)
        mixed = []
        for pair in range(pairs):
            tile, half = (pair // 2, pair % 2)
            lanes = slice(tile * LANES, (tile + 1) * LANES)
            query = q_ref[step, block * WINDOW : (block + 1) * WINDOW, pair * LANES : (pair + 1) * LANES]
            query = query.astype(jnp.float32) * HEAD_DIM**-0.5
            turned = pltpu.roll(query, HEAD_DIM, 1)
            if half == 0:
                both = (jnp.where(low, query, 0.0), jnp.where(low, turned, 0.0))
            else:
                both = (jnp.where(low, 0.0, turned), jnp.where(low, 0.0, query))
            query = jnp.concatenate(both, axis=0).astype(jnp.bfloat16)
            keys = kv_ref[0, pl.ds(start, 3 * WINDOW), lanes]
            values = kv_ref[1, pl.ds(start, 3 * WINDOW), lanes]
            scores = lax.dot_general(
                query, keys, (((1,), (1,)), ((), ())), preferred_element_type=jnp.float32
            )
            before = jnp.where(before_ok, scores[:, :WINDOW], NEG)
            middle = scores[:, WINDOW : 2 * WINDOW]
            after = jnp.where(after_ok, scores[:, 2 * WINDOW :], NEG)
            sink_col = jnp.where(upper, sink[2 * pair], sink[2 * pair + 1])
            top = jnp.max(
                jnp.maximum(jnp.maximum(before, after), middle), axis=-1, keepdims=True
            )
            top = jnp.maximum(top, sink_col)
            expd = jnp.concatenate(
                [jnp.exp(part - top).astype(jnp.bfloat16) for part in (before, middle, after)],
                axis=1,
            )
            summed = jnp.dot(
                expd,
                jnp.concatenate([values, ones], axis=1),
                preferred_element_type=jnp.float32,
            )
            result = summed[:, :LANES] / (summed[:, LANES:] + jnp.exp(sink_col - top))
            first, second = (result[:WINDOW], result[WINDOW:])
            if half == 0:
                second = pltpu.roll(second, HEAD_DIM, 1)
            else:
                first = pltpu.roll(first, HEAD_DIM, 1)
            mixed.append(jnp.where(low, first, second).astype(jnp.bfloat16))
        finished.append(jnp.concatenate(mixed, axis=1))
    attended = jnp.concatenate(finished, axis=0)

    @pl.when(step == 0)
    def _():
        weight_copy.wait()

    projected = jnp.dot(attended, weight_ref[...], preferred_element_type=jnp.float32).astype(
        jnp.bfloat16
    )
    half = rows // 2
    for turn in range(len(out_refs) // 2):

        @pl.when(step == turn)
        def _():
            out_refs[2 * turn][...] = projected[:half]
            out_refs[2 * turn + 1][...] = projected[half:]


def attend(sink, queries, before, middle, after, out_weight, rels, n_tp):
    tok_rows, width = queries.shape
    rows, steps = (tok_rows // n_tp, len(rels))
    cols = out_weight.shape[1]
    anywhere = pl.BlockSpec(memory_space=pl.ANY)
    hbm = pl.BlockSpec(memory_space=pltpu.HBM)
    return pl.pallas_call(
        functools.partial(attend_kernel, rels=rels),
        grid=(steps,),
        in_specs=[
            pl.BlockSpec(memory_space=pltpu.SMEM),
            hbm,
            anywhere,
            hbm,
            anywhere,
            hbm,
        ],
        out_specs=[pl.BlockSpec((rows // 2, cols), lambda i: (0, 0))] * (2 * steps),
        scratch_shapes=[
            pltpu.VMEM((steps, rows, width), jnp.bfloat16),
            pltpu.VMEM((2, tok_rows + 2 * WINDOW, middle.shape[2]), jnp.bfloat16),
            pltpu.VMEM(out_weight.shape, jnp.bfloat16),
            pltpu.SemaphoreType.DMA((4 + steps,)),
        ],
        out_shape=[jax.ShapeDtypeStruct((rows // 2, cols), jnp.bfloat16)] * (2 * steps),
        compiler_params=pltpu.CompilerParams(vmem_limit_bytes=52 * 1024 * 1024),
        name="attend",
    )(sink, queries, before, middle, after, out_weight)


def norm_kernel(*refs, tops, bottoms, outs, block):
    count = max(max(tops), max(bottoms)) + 1
    sources, (gain, bias), results = (refs[:count], refs[count : count + 2], refs[count + 2 : -3])
    parts, out, sems = refs[-3:]
    rows, width = out.shape
    steps = rows // block
    half = steps // 2

    def in_copy(step, place):
        ref = sources[(tops if step < half else bottoms)[place]]
        at = step * block % ref.shape[0]
        return pltpu.make_async_copy(
            ref.at[pl.ds(at, block)],
            parts.at[place, pl.ds(step * block, block)],
            sems.at[step * (len(tops) + 1) + place],
        )

    def out_copy(step):
        ref = results[step * block // (rows // outs)]
        at = step * block % ref.shape[0]
        return pltpu.make_async_copy(
            out.at[pl.ds(step * block, block)],
            ref.at[pl.ds(at, block)],
            sems.at[step * (len(tops) + 1) + len(tops)],
        )

    for step in range(steps):
        for place in range(len(tops)):
            in_copy(step, place).start()
    for step in range(steps):
        span = slice(step * block, (step + 1) * block)
        values = None
        for place in range(len(tops)):
            in_copy(step, place).wait()
        for place in range(len(tops)):
            part = parts[place, span].astype(jnp.float32)
            values = part if values is None else values + part
        mean = jnp.sum(values, axis=-1, keepdims=True) * (1.0 / width)
        centred = values - mean
        variance = jnp.sum(centred * centred, axis=-1, keepdims=True) * (1.0 / width)
        out[span] = (centred * lax.rsqrt(variance + 1e-06) * gain[...] + bias[...]).astype(
            jnp.bfloat16
        )
        out_copy(step).start()
    for step in range(steps):
        out_copy(step).wait()


def norm_rows(sources, tops, bottoms, outs, gain, bias, rows, block=64):
    width = sources[0].shape[1]
    anywhere = pl.BlockSpec(memory_space=pl.ANY)
    vmem = pl.BlockSpec(memory_space=pltpu.VMEM)
    steps = rows // block
    return pl.pallas_call(
        functools.partial(norm_kernel, tops=tops, bottoms=bottoms, outs=outs, block=block),
        in_specs=[anywhere] * len(sources) + [vmem, vmem],
        out_specs=[anywhere] * outs,
        out_shape=[jax.ShapeDtypeStruct((rows // outs, width), jnp.bfloat16)] * outs,
        scratch_shapes=[
            pltpu.VMEM((len(tops), rows, width), jnp.bfloat16),
            pltpu.VMEM((rows, width), jnp.bfloat16),
            pltpu.SemaphoreType.DMA((steps * (len(tops) + 1),)),
        ],
        compiler_params=pltpu.CompilerParams(vmem_limit_bytes=16 * 1024 * 1024),
        name="norm",
    )(*sources, gain[None], bias[None])


def added(part, arrived):
    return (part.astype(jnp.float32) + arrived.astype(jnp.float32)).astype(jnp.bfloat16)


def feed_kernel(*refs, count, outs, chunk):
    rows, weights, results = (refs[:count], refs[count], refs[count + 1 : count + 1 + outs])
    tokens, up, down, activation, branch, sems = refs[count + 1 + outs :]
    pieces, height, units = up.shape
    size, steps = (rows[0].shape[0], units // chunk)
    height_out = results[0].shape[0]
    part = pieces // steps
    width = part * height

    def row_copy(index):
        span = pl.ds(index * size, size)
        return pltpu.make_async_copy(rows[index], tokens.at[span], sems.at[2 * steps + index])

    def up_copy(k):
        cols = pl.ds(pl.multiple_of(k * chunk, chunk), chunk)
        return pltpu.make_async_copy(weights.at[:, 0, :, cols], up.at[:, :, cols], sems.at[k])

    def down_copy(k):
        span = pl.ds(k * part, part)
        return pltpu.make_async_copy(weights.at[span, 1], down.at[span], sems.at[steps + k])

    def out_copy(index, k):
        cols = pl.ds(pl.multiple_of(k * width, width), width)
        span = pl.ds(index * height_out, height_out)
        return pltpu.make_async_copy(
            branch.at[span, cols],
            results[index].at[:, cols],
            sems.at[2 * steps + count + index * steps + k],
        )

    for index in range(count):
        row_copy(index).start()
    for k in range(steps):
        up_copy(k).start()
    for k in range(steps):
        down_copy(k).start()
    for index in range(count):
        row_copy(index).wait()

    @pl.loop(0, steps)
    def _(k):
        up_copy(k).wait()
        cols = pl.ds(pl.multiple_of(k * chunk, chunk), chunk)
        hidden = jnp.dot(
            tokens[...],
            up[:, :, cols].reshape(pieces * height, chunk),
            preferred_element_type=jnp.float32,
        )
        activation[:, cols] = jnp.square(jnp.maximum(hidden, 0.0)).astype(jnp.bfloat16)

    @pl.loop(0, steps)
    def _(k):
        down_copy(k).wait()
        cols = pl.ds(pl.multiple_of(k * width, width), width)
        branch[:, cols] = lax.dot_general(
            activation[...],
            down[pl.ds(k * part, part)].reshape(width, units),
            (((1,), (1,)), ((), ())),
            preferred_element_type=jnp.float32,
        ).astype(jnp.bfloat16)
        for index in range(outs):
            out_copy(index, k).start()

    @pl.loop(0, steps)
    def _(k):
        for index in range(outs):
            out_copy(index, k).wait()


def feed_forward(rows, weights, height_out, chunk=512):
    size, width = rows[0].shape
    pieces, _, height, units = weights.shape
    count, total = (len(rows), len(rows) * size)
    outs = total // height_out
    anywhere = pl.BlockSpec(memory_space=pl.ANY)
    full = pltpu.VMEM((pieces, height, units), jnp.bfloat16)
    steps = units // chunk
    return pl.pallas_call(
        functools.partial(feed_kernel, count=count, outs=outs, chunk=chunk),
        in_specs=[anywhere] * (count + 1),
        out_specs=[anywhere] * outs,
        out_shape=[jax.ShapeDtypeStruct((height_out, width), jnp.bfloat16)] * outs,
        scratch_shapes=[
            pltpu.VMEM((total, width), jnp.bfloat16),
            full,
            full,
            pltpu.VMEM((total, units), jnp.bfloat16),
            pltpu.VMEM((total, width), jnp.bfloat16),
            pltpu.SemaphoreType.DMA((2 * steps + count + outs * steps,)),
        ],
        compiler_params=pltpu.CompilerParams(vmem_limit_bytes=40 * 1024 * 1024),
        name="feed",
    )(*rows, weights)


def layer(
    residual_in,
    queries,
    keys_values,
    sink_logit,
    out_weight,
    norm1_gain,
    norm1_bias,
    up_weight,
    down_weight,
    norm2_gain,
    norm2_bias,
):
    n_tp, n_sp = (lax.axis_size("tp"), lax.axis_size("sp"))
    shards, last, edge = prepare(up_weight, down_weight.T, keys_values)
    weights = lax.all_gather(shards, "sp", axis=0, tiled=True).reshape(
        n_sp, 2, up_weight.shape[0], up_weight.shape[1]
    )
    before, after = halo(last, edge, "sp")

    def run(*rels):
        return attend(
            sink_logit, queries, before, keys_values, after, out_weight, rels, n_tp
        )

    far_top, far_bottom = run(2)
    from_left = shift(far_top, 1)
    from_right = shift(far_bottom, -1)
    right_top, right_bottom, left_top, left_bottom = run(1, 3)
    left_plain = shift(right_bottom, 1)
    right_plain = shift(left_top, -1)
    own_top, own_bottom = run(0)
    left_sum = shift(added(right_top, from_left), 1)
    right_sum = shift(added(left_bottom, from_right), -1)
    rows, half = (2 * own_top.shape[0], own_top.shape[0])
    first_top, first_bottom = norm_rows(
        (residual_in, own_top, own_bottom, left_sum, left_plain, right_plain, right_sum),
        (0, 1, 3, 5),
        (0, 2, 4, 6),
        2,
        norm1_gain,
        norm1_bias,
        rows,
    )

    row_lt = shift(first_top, 1)
    row_rb = shift(first_bottom, -1)
    row_lb = shift(first_bottom, 1)
    row_rt = shift(first_top, -1)
    row_ft = shift(row_lt, 1)
    row_fb = shift(row_rb, -1)
    left_top, right_bottom = feed_forward((row_lt, row_rb), weights, half)
    left_plain = shift(right_bottom, 1)
    right_plain = shift(left_top, -1)
    far_top, far_bottom = feed_forward((row_ft, row_fb), weights, half)
    from_left = shift(far_top, 1)
    from_right = shift(far_bottom, -1)
    left_bottom, right_top = feed_forward((row_lb, row_rt), weights, half)
    left_sum = shift(added(right_top, from_left), 1)
    right_sum = shift(added(left_bottom, from_right), -1)
    own_top, own_bottom = feed_forward((first_top, first_bottom), weights, half)
    (out,) = norm_rows(
        (
            first_top,
            first_bottom,
            own_top,
            own_bottom,
            left_sum,
            left_plain,
            right_plain,
            right_sum,
        ),
        (0, 2, 4, 6),
        (1, 3, 5, 7),
        1,
        norm2_gain,
        norm2_bias,
        rows,
    )
    return out


def solution(mesh):
    return jax.shard_map(
        layer,
        mesh=mesh,
        in_specs=(
            P(("sp", "tp"), None),
            P("sp", "tp"),
            P(None, "sp", "tp"),
            P("tp"),
            P("tp", None),
            P(),
            P(),
            P("sp", "tp"),
            P("tp", "sp"),
            P(),
            P(),
        ),
        out_specs=P(("sp", "tp"), None),
        check_vma=False,
    )
```

```python
import functools

import jax
import jax.numpy as jnp
from jax import lax
from jax.experimental import pallas as pl
from jax.experimental.pallas import tpu as pltpu
from jax.sharding import PartitionSpec as P


HEAD_DIM = 64
WINDOW = 128
LANES = 128
NEG = -1e30


def shift(value, step, axis="tp"):
    devices = lax.axis_size(axis)
    return lax.ppermute(value, axis, [(i, (i + step) % devices) for i in range(devices)])


def prepare_kernel(up, down, keys_values, joined, last, first, weights, sems):
    height, tok_rows = (up.shape[0], keys_values.shape[1])
    into = [
        pltpu.make_async_copy(up, weights.at[pl.ds(0, height)], sems.at[0]),
        pltpu.make_async_copy(down, weights.at[pl.ds(height, height)], sems.at[1]),
    ]
    edges = [
        pltpu.make_async_copy(
            keys_values.at[:, pl.ds(tok_rows - WINDOW, WINDOW)], last, sems.at[2]
        ),
        pltpu.make_async_copy(keys_values.at[:, pl.ds(0, WINDOW)], first, sems.at[3]),
    ]
    for copy in into + edges:
        copy.start()
    for copy in into:
        copy.wait()
    out = pltpu.make_async_copy(weights, joined, sems.at[4])
    out.start()
    for copy in edges + [out]:
        copy.wait()


def prepare(up, down, keys_values):
    anywhere = pl.BlockSpec(memory_space=pl.ANY)
    vmem = pl.BlockSpec(memory_space=pltpu.VMEM)
    edge = jax.ShapeDtypeStruct((2, WINDOW, keys_values.shape[2]), jnp.bfloat16)
    both = (2 * up.shape[0], up.shape[1])
    return pl.pallas_call(
        prepare_kernel,
        in_specs=[anywhere] * 3,
        out_specs=[anywhere, vmem, vmem],
        out_shape=[jax.ShapeDtypeStruct(both, jnp.bfloat16), edge, edge],
        scratch_shapes=[pltpu.VMEM(both, jnp.bfloat16), pltpu.SemaphoreType.DMA((5,))],
        compiler_params=pltpu.CompilerParams(vmem_limit_bytes=60 * 1024 * 1024),
        name="prepare",
    )(up, down, keys_values)


def fetch_kernel(*refs):
    count = len(refs) // 2
    sems = refs[-1]
    copies = [
        pltpu.make_async_copy(refs[index], refs[count + index], sems.at[index])
        for index in range(count)
    ]
    for copy in copies:
        copy.start()
    for copy in copies:
        copy.wait()


def fetch(*arrays):
    anywhere = pl.BlockSpec(memory_space=pl.ANY)
    vmem = pl.BlockSpec(memory_space=pltpu.VMEM)
    return pl.pallas_call(
        fetch_kernel,
        in_specs=[anywhere] * len(arrays),
        out_specs=[anywhere] * len(arrays),
        out_shape=[jax.ShapeDtypeStruct(a.shape, a.dtype) for a in arrays],
        scratch_shapes=[pltpu.SemaphoreType.DMA((len(arrays),))],
        compiler_params=pltpu.CompilerParams(vmem_limit_bytes=47 * 1024 * 1024),
        name="fetch",
    )(*arrays)


def halo(last, first, axis):
    devices = lax.axis_size(axis)
    up = [(i, i + 1) for i in range(devices - 1)]
    down = [(j, i) for i, j in up]
    before = lax.ppermute(last, axis, up)
    after = lax.ppermute(first, axis, down)
    return before, after


def attend_kernel(sink, q_hbm, before_ref, mid_ref, after_ref, w_ref, *refs, rels):
    *out_refs, q_ref, kv_ref, weight_ref, sems = refs
    step = pl.program_id(0)
    rows, tok_rows = (q_ref.shape[1], mid_ref.shape[1])
    count = tok_rows // rows
    n_sp = lax.axis_size("sp")
    token_group, head_group = (lax.axis_index("sp"), lax.axis_index("tp"))
    rel = rels[-1]
    for turn in reversed(range(len(rels) - 1)):
        rel = jnp.where(step == turn, rels[turn], rel)
    quarter = (head_group + rel) % count
    copies = [
        pltpu.make_async_copy(ref, kv_ref.at[:, pl.ds(at, ref.shape[1])], sems.at[index])
        for index, (ref, at) in enumerate(
            ((before_ref, 0), (mid_ref, WINDOW), (after_ref, WINDOW + tok_rows))
        )
    ] + [
        pltpu.make_async_copy(
            q_hbm.at[pl.ds(pl.multiple_of((head_group + turn) % count * rows, rows), rows)],
            q_ref.at[index],
            sems.at[4 + index],
        )
        for index, turn in enumerate(rels)
    ]
    weight_copy = pltpu.make_async_copy(w_ref, weight_ref, sems.at[3])

    @pl.when(step == 0)
    def _():
        for copy in copies:
            copy.start()
        weight_copy.start()
        for copy in copies:
            copy.wait()

    blocks = rows // WINDOW
    pairs = q_ref.shape[2] // LANES
    row = lax.broadcasted_iota(jnp.int32, (2 * WINDOW, WINDOW), 0) % WINDOW
    col = lax.broadcasted_iota(jnp.int32, (2 * WINDOW, WINDOW), 1)
    low = lax.broadcasted_iota(jnp.int32, (WINDOW, LANES), 1) < HEAD_DIM
    upper = lax.broadcasted_iota(jnp.int32, (2 * WINDOW, 1), 0) < WINDOW
    ones = jnp.ones((3 * WINDOW, LANES), jnp.bfloat16)
    finished = []
    for block in range(blocks):
        index = quarter * blocks + block
        at_start = jnp.where((token_group == 0) & (index == 0), 4 * WINDOW, 0)
        at_end = jnp.where((token_group == n_sp - 1) & (index == tok_rows // WINDOW - 1), 4 * WINDOW, 0)
        before_ok = col - row >= at_start
        after_ok = row - col >= at_end
        start = pl.multiple_of(index * WINDOW, WINDOW)
        mixed = []
        for pair in range(pairs):
            tile, half = (pair // 2, pair % 2)
            lanes = slice(tile * LANES, (tile + 1) * LANES)
            query = q_ref[step, block * WINDOW : (block + 1) * WINDOW, pair * LANES : (pair + 1) * LANES]
            query = query.astype(jnp.float32) * HEAD_DIM**-0.5
            turned = pltpu.roll(query, HEAD_DIM, 1)
            if half == 0:
                both = (jnp.where(low, query, 0.0), jnp.where(low, turned, 0.0))
            else:
                both = (jnp.where(low, 0.0, turned), jnp.where(low, 0.0, query))
            query = jnp.concatenate(both, axis=0).astype(jnp.bfloat16)
            keys = kv_ref[0, pl.ds(start, 3 * WINDOW), lanes]
            values = kv_ref[1, pl.ds(start, 3 * WINDOW), lanes]
            scores = lax.dot_general(
                query, keys, (((1,), (1,)), ((), ())), preferred_element_type=jnp.float32
            )
            before = jnp.where(before_ok, scores[:, :WINDOW], NEG)
            middle = scores[:, WINDOW : 2 * WINDOW]
            after = jnp.where(after_ok, scores[:, 2 * WINDOW :], NEG)
            sink_col = jnp.where(upper, sink[2 * pair], sink[2 * pair + 1])
            top = jnp.max(
                jnp.maximum(jnp.maximum(before, after), middle), axis=-1, keepdims=True
            )
            top = jnp.maximum(top, sink_col)
            expd = jnp.concatenate(
                [jnp.exp(part - top).astype(jnp.bfloat16) for part in (before, middle, after)],
                axis=1,
            )
            summed = jnp.dot(
                expd,
                jnp.concatenate([values, ones], axis=1),
                preferred_element_type=jnp.float32,
            )
            result = summed[:, :LANES] / (summed[:, LANES:] + jnp.exp(sink_col - top))
            first, second = (result[:WINDOW], result[WINDOW:])
            if half == 0:
                second = pltpu.roll(second, HEAD_DIM, 1)
            else:
                first = pltpu.roll(first, HEAD_DIM, 1)
            mixed.append(jnp.where(low, first, second).astype(jnp.bfloat16))
        finished.append(jnp.concatenate(mixed, axis=1))
    attended = jnp.concatenate(finished, axis=0)

    @pl.when(step == 0)
    def _():
        weight_copy.wait()

    projected = jnp.dot(attended, weight_ref[...], preferred_element_type=jnp.float32).astype(
        jnp.bfloat16
    )
    half = rows // 2
    for turn in range(len(out_refs) // 2):

        @pl.when(step == turn)
        def _():
            out_refs[2 * turn][...] = projected[:half]
            out_refs[2 * turn + 1][...] = projected[half:]


def attend(sink, queries, before, middle, after, out_weight, rels, n_tp):
    tok_rows, width = queries.shape
    rows, steps = (tok_rows // n_tp, len(rels))
    cols = out_weight.shape[1]
    anywhere = pl.BlockSpec(memory_space=pl.ANY)
    hbm = pl.BlockSpec(memory_space=pltpu.HBM)
    return pl.pallas_call(
        functools.partial(attend_kernel, rels=rels),
        grid=(steps,),
        in_specs=[
            pl.BlockSpec(memory_space=pltpu.SMEM),
            hbm,
            anywhere,
            hbm,
            anywhere,
            hbm,
        ],
        out_specs=[pl.BlockSpec((rows // 2, cols), lambda i: (0, 0))] * (2 * steps),
        scratch_shapes=[
            pltpu.VMEM((steps, rows, width), jnp.bfloat16),
            pltpu.VMEM((2, tok_rows + 2 * WINDOW, middle.shape[2]), jnp.bfloat16),
            pltpu.VMEM(out_weight.shape, jnp.bfloat16),
            pltpu.SemaphoreType.DMA((4 + steps,)),
        ],
        out_shape=[jax.ShapeDtypeStruct((rows // 2, cols), jnp.bfloat16)] * (2 * steps),
        compiler_params=pltpu.CompilerParams(vmem_limit_bytes=24 * 1024 * 1024),
        name="attend",
    )(sink, queries, before, middle, after, out_weight)


def norm_kernel(*refs, tops, bottoms, outs, block):
    count = max(max(tops), max(bottoms)) + 1
    sources, (gain, bias), results = (refs[:count], refs[count : count + 2], refs[count + 2 : -3])
    parts, out, sems = refs[-3:]
    rows, width = out.shape
    steps = rows // block
    half = steps // 2

    def in_copy(step, place):
        ref = sources[(tops if step < half else bottoms)[place]]
        at = step * block % ref.shape[0]
        return pltpu.make_async_copy(
            ref.at[pl.ds(at, block)],
            parts.at[place, pl.ds(step * block, block)],
            sems.at[step * (len(tops) + 1) + place],
        )

    def out_copy(step):
        ref = results[step * block // (rows // outs)]
        at = step * block % ref.shape[0]
        return pltpu.make_async_copy(
            out.at[pl.ds(step * block, block)],
            ref.at[pl.ds(at, block)],
            sems.at[step * (len(tops) + 1) + len(tops)],
        )

    for step in range(steps):
        for place in range(len(tops)):
            in_copy(step, place).start()
    for step in range(steps):
        span = slice(step * block, (step + 1) * block)
        values = None
        for place in range(len(tops)):
            in_copy(step, place).wait()
        for place in range(len(tops)):
            part = parts[place, span].astype(jnp.float32)
            values = part if values is None else values + part
        mean = jnp.sum(values, axis=-1, keepdims=True) * (1.0 / width)
        centred = values - mean
        variance = jnp.sum(centred * centred, axis=-1, keepdims=True) * (1.0 / width)
        out[span] = (centred * lax.rsqrt(variance + 1e-06) * gain[...] + bias[...]).astype(
            jnp.bfloat16
        )
        out_copy(step).start()
    for step in range(steps):
        out_copy(step).wait()


def norm_rows(sources, tops, bottoms, outs, gain, bias, rows, block=64):
    width = sources[0].shape[1]
    anywhere = pl.BlockSpec(memory_space=pl.ANY)
    vmem = pl.BlockSpec(memory_space=pltpu.VMEM)
    steps = rows // block
    return pl.pallas_call(
        functools.partial(norm_kernel, tops=tops, bottoms=bottoms, outs=outs, block=block),
        in_specs=[anywhere] * len(sources) + [vmem, vmem],
        out_specs=[anywhere] * outs,
        out_shape=[jax.ShapeDtypeStruct((rows // outs, width), jnp.bfloat16)] * outs,
        scratch_shapes=[
            pltpu.VMEM((len(tops), rows, width), jnp.bfloat16),
            pltpu.VMEM((rows, width), jnp.bfloat16),
            pltpu.SemaphoreType.DMA((steps * (len(tops) + 1),)),
        ],
        compiler_params=pltpu.CompilerParams(vmem_limit_bytes=16 * 1024 * 1024),
        name="norm",
    )(*sources, gain[None], bias[None])


def added(part, arrived):
    return (part.astype(jnp.float32) + arrived.astype(jnp.float32)).astype(jnp.bfloat16)


def feed_kernel(*refs, count, outs, chunk):
    rows, weights, results = (refs[:count], refs[count], refs[count + 1 : count + 1 + outs])
    tokens, up, down, activation, branch, sems = refs[count + 1 + outs :]
    pieces, height, units = up.shape
    size, steps = (rows[0].shape[0], units // chunk)
    height_out = results[0].shape[0]
    part = pieces // steps
    width = part * height

    def row_copy(index):
        span = pl.ds(index * size, size)
        return pltpu.make_async_copy(rows[index], tokens.at[span], sems.at[2 * steps + index])

    def up_copy(k):
        cols = pl.ds(pl.multiple_of(k * chunk, chunk), chunk)
        return pltpu.make_async_copy(weights.at[:, 0, :, cols], up.at[:, :, cols], sems.at[k])

    def down_copy(k):
        span = pl.ds(k * part, part)
        return pltpu.make_async_copy(weights.at[span, 1], down.at[span], sems.at[steps + k])

    def out_copy(index, k):
        cols = pl.ds(pl.multiple_of(k * width, width), width)
        span = pl.ds(index * height_out, height_out)
        return pltpu.make_async_copy(
            branch.at[span, cols],
            results[index].at[:, cols],
            sems.at[2 * steps + count + index * steps + k],
        )

    for index in range(count):
        row_copy(index).start()
    for k in range(steps):
        up_copy(k).start()
    for k in range(steps):
        down_copy(k).start()
    for index in range(count):
        row_copy(index).wait()

    @pl.loop(0, steps)
    def _(k):
        up_copy(k).wait()
        cols = pl.ds(pl.multiple_of(k * chunk, chunk), chunk)
        hidden = jnp.dot(
            tokens[...],
            up[:, :, cols].reshape(pieces * height, chunk),
            preferred_element_type=jnp.float32,
        )
        activation[:, cols] = jnp.square(jnp.maximum(hidden, 0.0)).astype(jnp.bfloat16)

    @pl.loop(0, steps)
    def _(k):
        down_copy(k).wait()
        cols = pl.ds(pl.multiple_of(k * width, width), width)
        branch[:, cols] = lax.dot_general(
            activation[...],
            down[pl.ds(k * part, part)].reshape(width, units),
            (((1,), (1,)), ((), ())),
            preferred_element_type=jnp.float32,
        ).astype(jnp.bfloat16)
        for index in range(outs):
            out_copy(index, k).start()

    @pl.loop(0, steps)
    def _(k):
        for index in range(outs):
            out_copy(index, k).wait()


def feed_forward(rows, weights, height_out, chunk=512):
    size, width = rows[0].shape
    pieces, _, height, units = weights.shape
    count, total = (len(rows), len(rows) * size)
    outs = total // height_out
    anywhere = pl.BlockSpec(memory_space=pl.ANY)
    full = pltpu.VMEM((pieces, height, units), jnp.bfloat16)
    steps = units // chunk
    return pl.pallas_call(
        functools.partial(feed_kernel, count=count, outs=outs, chunk=chunk),
        in_specs=[anywhere] * (count + 1),
        out_specs=[anywhere] * outs,
        out_shape=[jax.ShapeDtypeStruct((height_out, width), jnp.bfloat16)] * outs,
        scratch_shapes=[
            pltpu.VMEM((total, width), jnp.bfloat16),
            full,
            full,
            pltpu.VMEM((total, units), jnp.bfloat16),
            pltpu.VMEM((total, width), jnp.bfloat16),
            pltpu.SemaphoreType.DMA((2 * steps + count + outs * steps,)),
        ],
        compiler_params=pltpu.CompilerParams(vmem_limit_bytes=40 * 1024 * 1024),
        name="feed",
    )(*rows, weights)


def layer(
    residual_in,
    queries,
    keys_values,
    sink_logit,
    out_weight,
    norm1_gain,
    norm1_bias,
    up_weight,
    down_weight,
    norm2_gain,
    norm2_bias,
):
    n_tp, n_sp = (lax.axis_size("tp"), lax.axis_size("sp"))
    shards, last, edge = prepare(up_weight, down_weight.T, keys_values)
    weights = lax.all_gather(shards, "sp", axis=0, tiled=True).reshape(
        n_sp, 2, up_weight.shape[0], up_weight.shape[1]
    )
    before, after = halo(last, edge, "sp")
    queries, keys_values, out_weight = fetch(queries, keys_values, out_weight)

    def run(*rels):
        return attend(
            sink_logit, queries, before, keys_values, after, out_weight, rels, n_tp
        )

    far_top, far_bottom = run(2)
    from_left = shift(far_top, 1)
    from_right = shift(far_bottom, -1)
    right_top, right_bottom, left_top, left_bottom = run(1, 3)
    left_plain = shift(right_bottom, 1)
    right_plain = shift(left_top, -1)
    own_top, own_bottom = run(0)
    left_sum = shift(added(right_top, from_left), 1)
    right_sum = shift(added(left_bottom, from_right), -1)
    rows, half = (2 * own_top.shape[0], own_top.shape[0])
    first_top, first_bottom = norm_rows(
        (residual_in, own_top, own_bottom, left_sum, left_plain, right_plain, right_sum),
        (0, 1, 3, 5),
        (0, 2, 4, 6),
        2,
        norm1_gain,
        norm1_bias,
        rows,
    )

    row_lt = shift(first_top, 1)
    row_rb = shift(first_bottom, -1)
    row_lb = shift(first_bottom, 1)
    row_rt = shift(first_top, -1)
    row_ft = shift(row_lt, 1)
    row_fb = shift(row_rb, -1)
    left_top, right_bottom = feed_forward((row_lt, row_rb), weights, half)
    left_plain = shift(right_bottom, 1)
    right_plain = shift(left_top, -1)
    far_top, far_bottom = feed_forward((row_ft, row_fb), weights, half)
    from_left = shift(far_top, 1)
    from_right = shift(far_bottom, -1)
    left_bottom, right_top = feed_forward((row_lb, row_rt), weights, half)
    left_sum = shift(added(right_top, from_left), 1)
    right_sum = shift(added(left_bottom, from_right), -1)
    own_top, own_bottom = feed_forward((first_top, first_bottom), weights, half)
    (out,) = norm_rows(
        (
            first_top,
            first_bottom,
            own_top,
            own_bottom,
            left_sum,
            left_plain,
            right_plain,
            right_sum,
        ),
        (0, 2, 4, 6),
        (1, 3, 5, 7),
        1,
        norm2_gain,
        norm2_bias,
        rows,
    )
    return out


def solution(mesh):
    return jax.shard_map(
        layer,
        mesh=mesh,
        in_specs=(
            P(("sp", "tp"), None),
            P("sp", "tp"),
            P(None, "sp", "tp"),
            P("tp"),
            P("tp", None),
            P(),
            P(),
            P("sp", "tp"),
            P("tp", "sp"),
            P(),
            P(),
        ),
        out_specs=P(("sp", "tp"), None),
        check_vma=False,
    )
```

```python
import functools

import jax
import jax.numpy as jnp
from jax import lax
from jax.experimental import pallas as pl
from jax.experimental.pallas import tpu as pltpu
from jax.sharding import PartitionSpec as P


HEAD_DIM = 64
WINDOW = 128
LANES = 128
NEG = -1e30


def shift(value, step, axis="tp"):
    devices = lax.axis_size(axis)
    return lax.ppermute(value, axis, [(i, (i + step) % devices) for i in range(devices)])


def prepare_kernel(up, down, keys_values, joined, last, first, weights, sems):
    height, tok_rows = (up.shape[0], keys_values.shape[1])
    into = [
        pltpu.make_async_copy(up, weights.at[pl.ds(0, height)], sems.at[0]),
        pltpu.make_async_copy(down, weights.at[pl.ds(height, height)], sems.at[1]),
    ]
    edges = [
        pltpu.make_async_copy(
            keys_values.at[:, pl.ds(tok_rows - WINDOW, WINDOW)], last, sems.at[2]
        ),
        pltpu.make_async_copy(keys_values.at[:, pl.ds(0, WINDOW)], first, sems.at[3]),
    ]
    for copy in into + edges:
        copy.start()
    for copy in into:
        copy.wait()
    out = pltpu.make_async_copy(weights, joined, sems.at[4])
    out.start()
    for copy in edges + [out]:
        copy.wait()


def prepare(up, down, keys_values):
    anywhere = pl.BlockSpec(memory_space=pl.ANY)
    vmem = pl.BlockSpec(memory_space=pltpu.VMEM)
    edge = jax.ShapeDtypeStruct((2, WINDOW, keys_values.shape[2]), jnp.bfloat16)
    both = (2 * up.shape[0], up.shape[1])
    return pl.pallas_call(
        prepare_kernel,
        in_specs=[anywhere] * 3,
        out_specs=[anywhere, vmem, vmem],
        out_shape=[jax.ShapeDtypeStruct(both, jnp.bfloat16), edge, edge],
        scratch_shapes=[pltpu.VMEM(both, jnp.bfloat16), pltpu.SemaphoreType.DMA((5,))],
        compiler_params=pltpu.CompilerParams(vmem_limit_bytes=60 * 1024 * 1024),
        name="prepare",
    )(up, down, keys_values)


def fetch_kernel(*refs):
    count = len(refs) // 2
    sems = refs[-1]
    copies = [
        pltpu.make_async_copy(refs[index], refs[count + index], sems.at[index])
        for index in range(count)
    ]
    for copy in copies:
        copy.start()
    for copy in copies:
        copy.wait()


def fetch(*arrays):
    anywhere = pl.BlockSpec(memory_space=pl.ANY)
    vmem = pl.BlockSpec(memory_space=pltpu.VMEM)
    return pl.pallas_call(
        fetch_kernel,
        in_specs=[anywhere] * len(arrays),
        out_specs=[anywhere] * len(arrays),
        out_shape=[jax.ShapeDtypeStruct(a.shape, a.dtype) for a in arrays],
        scratch_shapes=[pltpu.SemaphoreType.DMA((len(arrays),))],
        compiler_params=pltpu.CompilerParams(vmem_limit_bytes=47 * 1024 * 1024),
        name="fetch",
    )(*arrays)


def halo(last, first, axis):
    devices = lax.axis_size(axis)
    up = [(i, i + 1) for i in range(devices - 1)]
    down = [(j, i) for i, j in up]
    before = lax.ppermute(last, axis, up)
    after = lax.ppermute(first, axis, down)
    return before, after


def attend_kernel(sink, q_hbm, before_ref, mid_ref, after_ref, w_ref, *refs, rels):
    *out_refs, q_ref, kv_ref, weight_ref, sems = refs
    step = pl.program_id(0)
    rows, tok_rows = (q_ref.shape[1], mid_ref.shape[1])
    count = tok_rows // rows
    n_sp = lax.axis_size("sp")
    token_group, head_group = (lax.axis_index("sp"), lax.axis_index("tp"))
    rel = rels[-1]
    for turn in reversed(range(len(rels) - 1)):
        rel = jnp.where(step == turn, rels[turn], rel)
    quarter = (head_group + rel) % count
    copies = [
        pltpu.make_async_copy(ref, kv_ref.at[:, pl.ds(at, ref.shape[1])], sems.at[index])
        for index, (ref, at) in enumerate(
            ((before_ref, 0), (mid_ref, WINDOW), (after_ref, WINDOW + tok_rows))
        )
    ] + [
        pltpu.make_async_copy(
            q_hbm.at[pl.ds(pl.multiple_of((head_group + turn) % count * rows, rows), rows)],
            q_ref.at[index],
            sems.at[4 + index],
        )
        for index, turn in enumerate(rels)
    ]
    weight_copy = pltpu.make_async_copy(w_ref, weight_ref, sems.at[3])

    @pl.when(step == 0)
    def _():
        for copy in copies:
            copy.start()
        weight_copy.start()
        for copy in copies:
            copy.wait()

    blocks = rows // WINDOW
    pairs = q_ref.shape[2] // LANES
    row = lax.broadcasted_iota(jnp.int32, (2 * WINDOW, WINDOW), 0) % WINDOW
    col = lax.broadcasted_iota(jnp.int32, (2 * WINDOW, WINDOW), 1)
    low = lax.broadcasted_iota(jnp.int32, (WINDOW, LANES), 1) < HEAD_DIM
    upper = lax.broadcasted_iota(jnp.int32, (2 * WINDOW, 1), 0) < WINDOW
    ones = jnp.ones((3 * WINDOW, LANES), jnp.bfloat16)
    finished = []
    for block in range(blocks):
        index = quarter * blocks + block
        at_start = jnp.where((token_group == 0) & (index == 0), 4 * WINDOW, 0)
        at_end = jnp.where((token_group == n_sp - 1) & (index == tok_rows // WINDOW - 1), 4 * WINDOW, 0)
        before_ok = col - row >= at_start
        after_ok = row - col >= at_end
        start = pl.multiple_of(index * WINDOW, WINDOW)
        mixed = []
        for pair in range(pairs):
            tile, half = (pair // 2, pair % 2)
            lanes = slice(tile * LANES, (tile + 1) * LANES)
            query = q_ref[step, block * WINDOW : (block + 1) * WINDOW, pair * LANES : (pair + 1) * LANES]
            query = query.astype(jnp.float32) * HEAD_DIM**-0.5
            turned = pltpu.roll(query, HEAD_DIM, 1)
            if half == 0:
                both = (jnp.where(low, query, 0.0), jnp.where(low, turned, 0.0))
            else:
                both = (jnp.where(low, 0.0, turned), jnp.where(low, 0.0, query))
            query = jnp.concatenate(both, axis=0).astype(jnp.bfloat16)
            keys = kv_ref[0, pl.ds(start, 3 * WINDOW), lanes]
            values = kv_ref[1, pl.ds(start, 3 * WINDOW), lanes]
            scores = lax.dot_general(
                query, keys, (((1,), (1,)), ((), ())), preferred_element_type=jnp.float32
            )
            before = jnp.where(before_ok, scores[:, :WINDOW], NEG)
            middle = scores[:, WINDOW : 2 * WINDOW]
            after = jnp.where(after_ok, scores[:, 2 * WINDOW :], NEG)
            sink_col = jnp.where(upper, sink[2 * pair], sink[2 * pair + 1])
            top = jnp.max(
                jnp.maximum(jnp.maximum(before, after), middle), axis=-1, keepdims=True
            )
            top = jnp.maximum(top, sink_col)
            expd = jnp.concatenate(
                [jnp.exp(part - top).astype(jnp.bfloat16) for part in (before, middle, after)],
                axis=1,
            )
            summed = jnp.dot(
                expd,
                jnp.concatenate([values, ones], axis=1),
                preferred_element_type=jnp.float32,
            )
            result = summed[:, :LANES] / (summed[:, LANES:] + jnp.exp(sink_col - top))
            first, second = (result[:WINDOW], result[WINDOW:])
            if half == 0:
                second = pltpu.roll(second, HEAD_DIM, 1)
            else:
                first = pltpu.roll(first, HEAD_DIM, 1)
            mixed.append(jnp.where(low, first, second).astype(jnp.bfloat16))
        finished.append(jnp.concatenate(mixed, axis=1))
    attended = jnp.concatenate(finished, axis=0)

    @pl.when(step == 0)
    def _():
        weight_copy.wait()

    projected = jnp.dot(attended, weight_ref[...], preferred_element_type=jnp.float32).astype(
        jnp.bfloat16
    )
    half = rows // 2
    for turn in range(len(out_refs) // 2):

        @pl.when(step == turn)
        def _():
            out_refs[2 * turn][...] = projected[:half]
            out_refs[2 * turn + 1][...] = projected[half:]


def attend(sink, queries, before, middle, after, out_weight, rels, n_tp):
    tok_rows, width = queries.shape
    rows, steps = (tok_rows // n_tp, len(rels))
    cols = out_weight.shape[1]
    anywhere = pl.BlockSpec(memory_space=pl.ANY)
    hbm = pl.BlockSpec(memory_space=pltpu.HBM)
    return pl.pallas_call(
        functools.partial(attend_kernel, rels=rels),
        grid=(steps,),
        in_specs=[
            pl.BlockSpec(memory_space=pltpu.SMEM),
            hbm,
            anywhere,
            hbm,
            anywhere,
            hbm,
        ],
        out_specs=[pl.BlockSpec((rows // 2, cols), lambda i: (0, 0))] * (2 * steps),
        scratch_shapes=[
            pltpu.VMEM((steps, rows, width), jnp.bfloat16),
            pltpu.VMEM((2, tok_rows + 2 * WINDOW, middle.shape[2]), jnp.bfloat16),
            pltpu.VMEM(out_weight.shape, jnp.bfloat16),
            pltpu.SemaphoreType.DMA((4 + steps,)),
        ],
        out_shape=[jax.ShapeDtypeStruct((rows // 2, cols), jnp.bfloat16)] * (2 * steps),
        compiler_params=pltpu.CompilerParams(vmem_limit_bytes=24 * 1024 * 1024),
        name="attend",
    )(sink, queries, before, middle, after, out_weight)


def norm_kernel(*refs, tops, bottoms, outs, block):
    count = max(max(tops), max(bottoms)) + 1
    sources, (gain, bias), results = (refs[:count], refs[count : count + 2], refs[count + 2 : -3])
    parts, out, sems = refs[-3:]
    rows, width = out.shape
    steps = rows // block
    half = steps // 2

    def in_copy(step, place):
        ref = sources[(tops if step < half else bottoms)[place]]
        at = step * block % ref.shape[0]
        return pltpu.make_async_copy(
            ref.at[pl.ds(at, block)],
            parts.at[place, pl.ds(step * block, block)],
            sems.at[step * (len(tops) + 1) + place],
        )

    def out_copy(step):
        ref = results[step * block // (rows // outs)]
        at = step * block % ref.shape[0]
        return pltpu.make_async_copy(
            out.at[pl.ds(step * block, block)],
            ref.at[pl.ds(at, block)],
            sems.at[step * (len(tops) + 1) + len(tops)],
        )

    for step in range(steps):
        for place in range(len(tops)):
            in_copy(step, place).start()
    for step in range(steps):
        span = slice(step * block, (step + 1) * block)
        values = None
        for place in range(len(tops)):
            in_copy(step, place).wait()
        for place in range(len(tops)):
            part = parts[place, span].astype(jnp.float32)
            values = part if values is None else values + part
        mean = jnp.sum(values, axis=-1, keepdims=True) * (1.0 / width)
        centred = values - mean
        variance = jnp.sum(centred * centred, axis=-1, keepdims=True) * (1.0 / width)
        out[span] = (centred * lax.rsqrt(variance + 1e-06) * gain[...] + bias[...]).astype(
            jnp.bfloat16
        )
        out_copy(step).start()
    for step in range(steps):
        out_copy(step).wait()


def norm_rows(sources, tops, bottoms, outs, gain, bias, rows, block=64):
    width = sources[0].shape[1]
    anywhere = pl.BlockSpec(memory_space=pl.ANY)
    vmem = pl.BlockSpec(memory_space=pltpu.VMEM)
    steps = rows // block
    return pl.pallas_call(
        functools.partial(norm_kernel, tops=tops, bottoms=bottoms, outs=outs, block=block),
        in_specs=[anywhere] * len(sources) + [vmem, vmem],
        out_specs=[anywhere] * outs,
        out_shape=[jax.ShapeDtypeStruct((rows // outs, width), jnp.bfloat16)] * outs,
        scratch_shapes=[
            pltpu.VMEM((len(tops), rows, width), jnp.bfloat16),
            pltpu.VMEM((rows, width), jnp.bfloat16),
            pltpu.SemaphoreType.DMA((steps * (len(tops) + 1),)),
        ],
        compiler_params=pltpu.CompilerParams(vmem_limit_bytes=16 * 1024 * 1024),
        name="norm",
    )(*sources, gain[None], bias[None])


def added(part, arrived):
    return (part.astype(jnp.float32) + arrived.astype(jnp.float32)).astype(jnp.bfloat16)


def feed_kernel(*refs, count, chunk, resident):
    rows, rest = (refs[:count], refs[count:])
    if resident:
        up, down, *rest = rest
    else:
        weights, *rest = rest
    results, rest = (rest[:count], rest[count:])
    if not resident:
        up, down, *rest = rest
    tokens, activation, branch, sems, *load_sems = rest
    pieces, height, units = up.shape
    size, steps = (rows[0].shape[0], units // chunk)
    part = pieces // steps
    width = part * height

    def row_copy(index):
        span = pl.ds(index * size, size)
        return pltpu.make_async_copy(rows[index], tokens.at[span], sems.at[index])

    def up_copy(k):
        cols = pl.ds(pl.multiple_of(k * chunk, chunk), chunk)
        return pltpu.make_async_copy(
            weights.at[:, 0, :, cols], up.at[:, :, cols], load_sems[0].at[k]
        )

    def down_copy(k):
        span = pl.ds(k * part, part)
        return pltpu.make_async_copy(
            weights.at[span, 1], down.at[span], load_sems[0].at[steps + k]
        )

    def out_copy(index, k):
        cols = pl.ds(pl.multiple_of(k * width, width), width)
        span = pl.ds(index * size, size)
        return pltpu.make_async_copy(
            branch.at[span, cols], results[index].at[:, cols], sems.at[count + index * steps + k]
        )

    for index in range(count):
        row_copy(index).start()
    if not resident:
        for k in range(steps):
            up_copy(k).start()
        for k in range(steps):
            down_copy(k).start()
    for index in range(count):
        row_copy(index).wait()

    @pl.loop(0, steps)
    def _(k):
        if not resident:
            up_copy(k).wait()
        cols = pl.ds(pl.multiple_of(k * chunk, chunk), chunk)
        hidden = jnp.dot(
            tokens[...],
            up[:, :, cols].reshape(pieces * height, chunk),
            preferred_element_type=jnp.float32,
        )
        activation[:, cols] = jnp.square(jnp.maximum(hidden, 0.0)).astype(jnp.bfloat16)

    @pl.loop(0, steps)
    def _(k):
        if not resident:
            down_copy(k).wait()
        cols = pl.ds(pl.multiple_of(k * width, width), width)
        branch[:, cols] = lax.dot_general(
            activation[...],
            down[pl.ds(k * part, part)].reshape(width, units),
            (((1,), (1,)), ((), ())),
            preferred_element_type=jnp.float32,
        ).astype(jnp.bfloat16)
        for index in range(count):
            out_copy(index, k).start()

    @pl.loop(0, steps)
    def _(k):
        for index in range(count):
            out_copy(index, k).wait()


def feed_forward(rows, weights):
    resident = len(weights) == 2
    chunk = 1024 if resident else 512
    size, width = rows[0].shape
    count, total = (len(rows), len(rows) * rows[0].shape[0])
    if resident:
        pieces, height, units = weights[0].shape
    else:
        pieces, _, height, units = weights[0].shape
    steps = units // chunk
    anywhere = pl.BlockSpec(memory_space=pl.ANY)
    vmem = pl.BlockSpec(memory_space=pltpu.VMEM)
    held = [] if resident else [jax.ShapeDtypeStruct((pieces, height, units), jnp.bfloat16)] * 2
    load_sems = [] if resident else [pltpu.SemaphoreType.DMA((2 * steps,))]
    return pl.pallas_call(
        functools.partial(feed_kernel, count=count, chunk=chunk, resident=resident),
        in_specs=[anywhere] * count + ([vmem] * 2 if resident else [anywhere]),
        out_specs=[anywhere] * count + [vmem] * len(held),
        out_shape=[jax.ShapeDtypeStruct((size, width), jnp.bfloat16)] * count + held,
        scratch_shapes=[
            pltpu.VMEM((total, width), jnp.bfloat16),
            pltpu.VMEM((total, units), jnp.bfloat16),
            pltpu.VMEM((total, width), jnp.bfloat16),
            pltpu.SemaphoreType.DMA((count + count * steps,)),
            *load_sems,
        ],
        compiler_params=pltpu.CompilerParams(
            vmem_limit_bytes=(12 if resident else 32) * 1024 * 1024
        ),
        name="feed",
    )(*rows, *weights)


def layer(
    residual_in,
    queries,
    keys_values,
    sink_logit,
    out_weight,
    norm1_gain,
    norm1_bias,
    up_weight,
    down_weight,
    norm2_gain,
    norm2_bias,
):
    n_tp, n_sp = (lax.axis_size("tp"), lax.axis_size("sp"))
    shards, last, edge = prepare(up_weight, down_weight.T, keys_values)
    weights = lax.all_gather(shards, "sp", axis=0, tiled=True).reshape(
        n_sp, 2, up_weight.shape[0], up_weight.shape[1]
    )
    before, after = halo(last, edge, "sp")
    queries, keys_values, out_weight = fetch(queries, keys_values, out_weight)

    def run(*rels):
        return attend(
            sink_logit, queries, before, keys_values, after, out_weight, rels, n_tp
        )

    far_top, far_bottom = run(2)
    from_left = shift(far_top, 1)
    from_right = shift(far_bottom, -1)
    right_top, right_bottom, left_top, left_bottom = run(1, 3)
    left_plain = shift(right_bottom, 1)
    right_plain = shift(left_top, -1)
    own_top, own_bottom = run(0)
    left_sum = shift(added(right_top, from_left), 1)
    right_sum = shift(added(left_bottom, from_right), -1)
    rows = 2 * own_top.shape[0]
    first_top, first_bottom = norm_rows(
        (residual_in, own_top, own_bottom, left_sum, left_plain, right_plain, right_sum),
        (0, 1, 3, 5),
        (0, 2, 4, 6),
        2,
        norm1_gain,
        norm1_bias,
        rows,
    )

    row_lt = shift(first_top, 1)
    row_rb = shift(first_bottom, -1)
    row_lb = shift(first_bottom, 1)
    row_rt = shift(first_top, -1)
    row_ft = shift(row_lt, 1)
    row_fb = shift(row_rb, -1)
    left_top, right_bottom, *held = feed_forward((row_lt, row_rb), (weights,))
    left_plain = shift(right_bottom, 1)
    right_plain = shift(left_top, -1)
    far_top, far_bottom = feed_forward((row_ft, row_fb), held)
    from_left = shift(far_top, 1)
    from_right = shift(far_bottom, -1)
    left_bottom, right_top = feed_forward((row_lb, row_rt), held)
    left_sum = shift(added(right_top, from_left), 1)
    right_sum = shift(added(left_bottom, from_right), -1)
    own_top, own_bottom = feed_forward((first_top, first_bottom), held)
    (out,) = norm_rows(
        (
            first_top,
            first_bottom,
            own_top,
            own_bottom,
            left_sum,
            left_plain,
            right_plain,
            right_sum,
        ),
        (0, 2, 4, 6),
        (1, 3, 5, 7),
        1,
        norm2_gain,
        norm2_bias,
        rows,
    )
    return out


def solution(mesh):
    return jax.shard_map(
        layer,
        mesh=mesh,
        in_specs=(
            P(("sp", "tp"), None),
            P("sp", "tp"),
            P(None, "sp", "tp"),
            P("tp"),
            P("tp", None),
            P(),
            P(),
            P("sp", "tp"),
            P("tp", "sp"),
            P(),
            P(),
        ),
        out_specs=P(("sp", "tp"), None),
        check_vma=False,
    )
```

```python
import functools

import jax
import jax.numpy as jnp
from jax import lax
from jax.experimental import pallas as pl
from jax.experimental.pallas import tpu as pltpu
from jax.sharding import PartitionSpec as P


HEAD_DIM = 64
WINDOW = 128
LANES = 128
NEG = -1e30


def shift(value, step, axis="tp"):
    devices = lax.axis_size(axis)
    return lax.ppermute(value, axis, [(i, (i + step) % devices) for i in range(devices)])


def prepare_kernel(up, down, keys_values, joined, last, first, weights, sems):
    height, tok_rows = (up.shape[0], keys_values.shape[1])
    into = [
        pltpu.make_async_copy(up, weights.at[pl.ds(0, height)], sems.at[0]),
        pltpu.make_async_copy(down, weights.at[pl.ds(height, height)], sems.at[1]),
    ]
    edges = [
        pltpu.make_async_copy(
            keys_values.at[:, pl.ds(tok_rows - WINDOW, WINDOW)], last, sems.at[2]
        ),
        pltpu.make_async_copy(keys_values.at[:, pl.ds(0, WINDOW)], first, sems.at[3]),
    ]
    for copy in into + edges:
        copy.start()
    for copy in into:
        copy.wait()
    out = pltpu.make_async_copy(weights, joined, sems.at[4])
    out.start()
    for copy in edges + [out]:
        copy.wait()


def prepare(up, down, keys_values):
    anywhere = pl.BlockSpec(memory_space=pl.ANY)
    vmem = pl.BlockSpec(memory_space=pltpu.VMEM)
    edge = jax.ShapeDtypeStruct((2, WINDOW, keys_values.shape[2]), jnp.bfloat16)
    both = (2 * up.shape[0], up.shape[1])
    return pl.pallas_call(
        prepare_kernel,
        in_specs=[anywhere] * 3,
        out_specs=[anywhere, vmem, vmem],
        out_shape=[jax.ShapeDtypeStruct(both, jnp.bfloat16), edge, edge],
        scratch_shapes=[pltpu.VMEM(both, jnp.bfloat16), pltpu.SemaphoreType.DMA((5,))],
        compiler_params=pltpu.CompilerParams(vmem_limit_bytes=60 * 1024 * 1024),
        name="prepare",
    )(up, down, keys_values)


def fetch_kernel(*refs):
    count = len(refs) // 2
    sems = refs[-1]
    copies = [
        pltpu.make_async_copy(refs[index], refs[count + index], sems.at[index])
        for index in range(count)
    ]
    for copy in copies:
        copy.start()
    for copy in copies:
        copy.wait()


def fetch(*arrays):
    anywhere = pl.BlockSpec(memory_space=pl.ANY)
    vmem = pl.BlockSpec(memory_space=pltpu.VMEM)
    return pl.pallas_call(
        fetch_kernel,
        in_specs=[anywhere] * len(arrays),
        out_specs=[anywhere] * len(arrays),
        out_shape=[jax.ShapeDtypeStruct(a.shape, a.dtype) for a in arrays],
        scratch_shapes=[pltpu.SemaphoreType.DMA((len(arrays),))],
        compiler_params=pltpu.CompilerParams(vmem_limit_bytes=47 * 1024 * 1024),
        name="fetch",
    )(*arrays)


def halo(last, first, axis):
    devices = lax.axis_size(axis)
    up = [(i, i + 1) for i in range(devices - 1)]
    down = [(j, i) for i, j in up]
    before = lax.ppermute(last, axis, up)
    after = lax.ppermute(first, axis, down)
    return before, after


def attend_kernel(sink, q_hbm, before_ref, mid_ref, after_ref, w_ref, *refs, rels):
    *out_refs, q_ref, kv_ref, weight_ref, sems = refs
    step = pl.program_id(0)
    rows, tok_rows = (q_ref.shape[1], mid_ref.shape[1])
    count = tok_rows // rows
    n_sp = lax.axis_size("sp")
    token_group, head_group = (lax.axis_index("sp"), lax.axis_index("tp"))
    rel = rels[-1]
    for turn in reversed(range(len(rels) - 1)):
        rel = jnp.where(step == turn, rels[turn], rel)
    quarter = (head_group + rel) % count
    copies = [
        pltpu.make_async_copy(ref, kv_ref.at[:, pl.ds(at, ref.shape[1])], sems.at[index])
        for index, (ref, at) in enumerate(
            ((before_ref, 0), (mid_ref, WINDOW), (after_ref, WINDOW + tok_rows))
        )
    ] + [
        pltpu.make_async_copy(
            q_hbm.at[pl.ds(pl.multiple_of((head_group + turn) % count * rows, rows), rows)],
            q_ref.at[index],
            sems.at[4 + index],
        )
        for index, turn in enumerate(rels)
    ]
    weight_copy = pltpu.make_async_copy(w_ref, weight_ref, sems.at[3])

    @pl.when(step == 0)
    def _():
        for copy in copies:
            copy.start()
        weight_copy.start()
        for copy in copies:
            copy.wait()

    blocks = rows // WINDOW
    pairs = q_ref.shape[2] // LANES
    row = lax.broadcasted_iota(jnp.int32, (2 * WINDOW, WINDOW), 0) % WINDOW
    col = lax.broadcasted_iota(jnp.int32, (2 * WINDOW, WINDOW), 1)
    low = lax.broadcasted_iota(jnp.int32, (WINDOW, LANES), 1) < HEAD_DIM
    upper = lax.broadcasted_iota(jnp.int32, (2 * WINDOW, 1), 0) < WINDOW
    ones = jnp.ones((3 * WINDOW, LANES), jnp.bfloat16)
    finished = []
    for block in range(blocks):
        index = quarter * blocks + block
        at_start = jnp.where((token_group == 0) & (index == 0), 4 * WINDOW, 0)
        at_end = jnp.where((token_group == n_sp - 1) & (index == tok_rows // WINDOW - 1), 4 * WINDOW, 0)
        before_ok = col - row >= at_start
        after_ok = row - col >= at_end
        start = pl.multiple_of(index * WINDOW, WINDOW)
        mixed = []
        for pair in range(pairs):
            tile, half = (pair // 2, pair % 2)
            lanes = slice(tile * LANES, (tile + 1) * LANES)
            query = q_ref[step, block * WINDOW : (block + 1) * WINDOW, pair * LANES : (pair + 1) * LANES]
            query = query.astype(jnp.float32) * HEAD_DIM**-0.5
            turned = pltpu.roll(query, HEAD_DIM, 1)
            if half == 0:
                both = (jnp.where(low, query, 0.0), jnp.where(low, turned, 0.0))
            else:
                both = (jnp.where(low, 0.0, turned), jnp.where(low, 0.0, query))
            query = jnp.concatenate(both, axis=0).astype(jnp.bfloat16)
            keys = kv_ref[0, pl.ds(start, 3 * WINDOW), lanes]
            values = kv_ref[1, pl.ds(start, 3 * WINDOW), lanes]
            scores = lax.dot_general(
                query, keys, (((1,), (1,)), ((), ())), preferred_element_type=jnp.float32
            )
            before = jnp.where(before_ok, scores[:, :WINDOW], NEG)
            middle = scores[:, WINDOW : 2 * WINDOW]
            after = jnp.where(after_ok, scores[:, 2 * WINDOW :], NEG)
            sink_col = jnp.where(upper, sink[2 * pair], sink[2 * pair + 1])
            top = jnp.max(
                jnp.maximum(jnp.maximum(before, after), middle), axis=-1, keepdims=True
            )
            top = jnp.maximum(top, sink_col)
            expd = jnp.concatenate(
                [jnp.exp(part - top).astype(jnp.bfloat16) for part in (before, middle, after)],
                axis=1,
            )
            summed = jnp.dot(
                expd,
                jnp.concatenate([values, ones], axis=1),
                preferred_element_type=jnp.float32,
            )
            result = summed[:, :LANES] / (summed[:, LANES:] + jnp.exp(sink_col - top))
            first, second = (result[:WINDOW], result[WINDOW:])
            if half == 0:
                second = pltpu.roll(second, HEAD_DIM, 1)
            else:
                first = pltpu.roll(first, HEAD_DIM, 1)
            mixed.append(jnp.where(low, first, second).astype(jnp.bfloat16))
        finished.append(jnp.concatenate(mixed, axis=1))
    attended = jnp.concatenate(finished, axis=0)

    @pl.when(step == 0)
    def _():
        weight_copy.wait()

    projected = jnp.dot(attended, weight_ref[...], preferred_element_type=jnp.float32).astype(
        jnp.bfloat16
    )
    half = rows // 2
    for turn in range(len(out_refs) // 2):

        @pl.when(step == turn)
        def _():
            out_refs[2 * turn][...] = projected[:half]
            out_refs[2 * turn + 1][...] = projected[half:]


def attend(sink, queries, before, middle, after, out_weight, rels, n_tp):
    tok_rows, width = queries.shape
    rows, steps = (tok_rows // n_tp, len(rels))
    cols = out_weight.shape[1]
    anywhere = pl.BlockSpec(memory_space=pl.ANY)
    hbm = pl.BlockSpec(memory_space=pltpu.HBM)
    return pl.pallas_call(
        functools.partial(attend_kernel, rels=rels),
        grid=(steps,),
        in_specs=[
            pl.BlockSpec(memory_space=pltpu.SMEM),
            hbm,
            anywhere,
            hbm,
            anywhere,
            hbm,
        ],
        out_specs=[pl.BlockSpec((rows // 2, cols), lambda i: (0, 0))] * (2 * steps),
        scratch_shapes=[
            pltpu.VMEM((steps, rows, width), jnp.bfloat16),
            pltpu.VMEM((2, tok_rows + 2 * WINDOW, middle.shape[2]), jnp.bfloat16),
            pltpu.VMEM(out_weight.shape, jnp.bfloat16),
            pltpu.SemaphoreType.DMA((4 + steps,)),
        ],
        out_shape=[jax.ShapeDtypeStruct((rows // 2, cols), jnp.bfloat16)] * (2 * steps),
        compiler_params=pltpu.CompilerParams(vmem_limit_bytes=24 * 1024 * 1024),
        name="attend",
    )(sink, queries, before, middle, after, out_weight)


def norm_kernel(*refs, count, base, block):
    sources, (gain, bias) = (refs[:count], refs[count : count + 2])
    result, parts, out, sems = refs[-4:]
    rows, width = out.shape
    steps = rows // block

    def in_copy(step, place):
        ref = sources[place]
        at = (base + step * block) % ref.shape[0]
        return pltpu.make_async_copy(
            ref.at[pl.ds(at, block)],
            parts.at[place, pl.ds(step * block, block)],
            sems.at[step * (count + 1) + place],
        )

    def out_copy(step):
        at = (base + step * block) % result.shape[0]
        return pltpu.make_async_copy(
            out.at[pl.ds(step * block, block)],
            result.at[pl.ds(at, block)],
            sems.at[step * (count + 1) + count],
        )

    for step in range(steps):
        for place in range(count):
            in_copy(step, place).start()
    for step in range(steps):
        span = slice(step * block, (step + 1) * block)
        values = None
        for place in range(count):
            in_copy(step, place).wait()
        for place in range(count):
            part = parts[place, span].astype(jnp.float32)
            values = part if values is None else values + part
        mean = jnp.sum(values, axis=-1, keepdims=True) * (1.0 / width)
        centred = values - mean
        variance = jnp.sum(centred * centred, axis=-1, keepdims=True) * (1.0 / width)
        out[span] = (centred * lax.rsqrt(variance + 1e-06) * gain[...] + bias[...]).astype(
            jnp.bfloat16
        )
        out_copy(step).start()
    for step in range(steps):
        out_copy(step).wait()


def norm_half(sources, base, gain, bias, rows, out_rows, into=None, block=64):
    count, width = (len(sources), sources[0].shape[1])
    anywhere = pl.BlockSpec(memory_space=pl.ANY)
    vmem = pl.BlockSpec(memory_space=pltpu.VMEM)
    steps = rows // block
    extra = () if into is None else (into,)
    return pl.pallas_call(
        functools.partial(norm_kernel, count=count, base=base, block=block),
        in_specs=[anywhere] * count + [vmem, vmem] + [anywhere] * len(extra),
        out_specs=anywhere,
        out_shape=jax.ShapeDtypeStruct((out_rows, width), jnp.bfloat16),
        scratch_shapes=[
            pltpu.VMEM((count, rows, width), jnp.bfloat16),
            pltpu.VMEM((rows, width), jnp.bfloat16),
            pltpu.SemaphoreType.DMA((steps * (count + 1),)),
        ],
        input_output_aliases={count + 2: 0} if extra else {},
        compiler_params=pltpu.CompilerParams(vmem_limit_bytes=16 * 1024 * 1024),
        name="norm",
    )(*sources, gain[None], bias[None], *extra)


def added(part, arrived):
    return (part.astype(jnp.float32) + arrived.astype(jnp.float32)).astype(jnp.bfloat16)


def feed_kernel(*refs, count, chunk, resident):
    rows, rest = (refs[:count], refs[count:])
    if resident:
        up, down, *rest = rest
    else:
        weights, *rest = rest
    results, rest = (rest[:count], rest[count:])
    if not resident:
        up, down, *rest = rest
    tokens, activation, branch, sems, *load_sems = rest
    pieces, height, units = up.shape
    size, steps = (rows[0].shape[0], units // chunk)
    part = pieces // steps
    width = part * height

    def row_copy(index):
        span = pl.ds(index * size, size)
        return pltpu.make_async_copy(rows[index], tokens.at[span], sems.at[index])

    def up_copy(k):
        cols = pl.ds(pl.multiple_of(k * chunk, chunk), chunk)
        return pltpu.make_async_copy(
            weights.at[:, 0, :, cols], up.at[:, :, cols], load_sems[0].at[k]
        )

    def down_copy(k):
        span = pl.ds(k * part, part)
        return pltpu.make_async_copy(
            weights.at[span, 1], down.at[span], load_sems[0].at[steps + k]
        )

    def out_copy(index, k):
        cols = pl.ds(pl.multiple_of(k * width, width), width)
        span = pl.ds(index * size, size)
        return pltpu.make_async_copy(
            branch.at[span, cols], results[index].at[:, cols], sems.at[count + index * steps + k]
        )

    for index in range(count):
        row_copy(index).start()
    if not resident:
        for k in range(steps):
            up_copy(k).start()
        for k in range(steps):
            down_copy(k).start()
    for index in range(count):
        row_copy(index).wait()

    @pl.loop(0, steps)
    def _(k):
        if not resident:
            up_copy(k).wait()
        cols = pl.ds(pl.multiple_of(k * chunk, chunk), chunk)
        hidden = jnp.dot(
            tokens[...],
            up[:, :, cols].reshape(pieces * height, chunk),
            preferred_element_type=jnp.float32,
        )
        activation[:, cols] = jnp.square(jnp.maximum(hidden, 0.0)).astype(jnp.bfloat16)

    @pl.loop(0, steps)
    def _(k):
        if not resident:
            down_copy(k).wait()
        cols = pl.ds(pl.multiple_of(k * width, width), width)
        branch[:, cols] = lax.dot_general(
            activation[...],
            down[pl.ds(k * part, part)].reshape(width, units),
            (((1,), (1,)), ((), ())),
            preferred_element_type=jnp.float32,
        ).astype(jnp.bfloat16)
        for index in range(count):
            out_copy(index, k).start()

    @pl.loop(0, steps)
    def _(k):
        for index in range(count):
            out_copy(index, k).wait()


def feed_forward(rows, weights):
    resident = len(weights) == 2
    chunk = 1024 if resident else 512
    size, width = rows[0].shape
    count, total = (len(rows), len(rows) * rows[0].shape[0])
    if resident:
        pieces, height, units = weights[0].shape
    else:
        pieces, _, height, units = weights[0].shape
    steps = units // chunk
    anywhere = pl.BlockSpec(memory_space=pl.ANY)
    vmem = pl.BlockSpec(memory_space=pltpu.VMEM)
    held = [] if resident else [jax.ShapeDtypeStruct((pieces, height, units), jnp.bfloat16)] * 2
    load_sems = [] if resident else [pltpu.SemaphoreType.DMA((2 * steps,))]
    return pl.pallas_call(
        functools.partial(feed_kernel, count=count, chunk=chunk, resident=resident),
        in_specs=[anywhere] * count + ([vmem] * 2 if resident else [anywhere]),
        out_specs=[anywhere] * count + [vmem] * len(held),
        out_shape=[jax.ShapeDtypeStruct((size, width), jnp.bfloat16)] * count + held,
        scratch_shapes=[
            pltpu.VMEM((total, width), jnp.bfloat16),
            pltpu.VMEM((total, units), jnp.bfloat16),
            pltpu.VMEM((total, width), jnp.bfloat16),
            pltpu.SemaphoreType.DMA((count + count * steps,)),
            *load_sems,
        ],
        compiler_params=pltpu.CompilerParams(
            vmem_limit_bytes=(24 if resident else 32) * 1024 * 1024
        ),
        name="feed",
    )(*rows, *weights)


def layer(
    residual_in,
    queries,
    keys_values,
    sink_logit,
    out_weight,
    norm1_gain,
    norm1_bias,
    up_weight,
    down_weight,
    norm2_gain,
    norm2_bias,
):
    n_tp, n_sp = (lax.axis_size("tp"), lax.axis_size("sp"))
    shards, last, edge = prepare(up_weight, down_weight.T, keys_values)
    weights = lax.all_gather(shards, "sp", axis=0, tiled=True).reshape(
        n_sp, 2, up_weight.shape[0], up_weight.shape[1]
    )
    before, after = halo(last, edge, "sp")
    queries, keys_values, out_weight = fetch(queries, keys_values, out_weight)

    def run(*rels):
        return attend(
            sink_logit, queries, before, keys_values, after, out_weight, rels, n_tp
        )

    far_top, far_bottom = run(2)
    from_left = shift(far_top, 1)
    from_right = shift(far_bottom, -1)
    right_top, right_bottom, left_top, left_bottom = run(1, 3)
    left_plain = shift(right_bottom, 1)
    right_plain = shift(left_top, -1)
    own_top, own_bottom = run(0)
    left_sum = shift(added(right_top, from_left), 1)
    right_sum = shift(added(left_bottom, from_right), -1)
    rows, half = (2 * own_top.shape[0], own_top.shape[0])
    first_top = norm_half(
        (residual_in, own_top, left_sum, right_plain), 0, norm1_gain, norm1_bias, half, half
    )
    first_bottom = norm_half(
        (residual_in, own_bottom, left_plain, right_sum), half, norm1_gain, norm1_bias, half, half
    )

    row_lt = shift(first_top, 1)
    row_rb = shift(first_bottom, -1)
    row_lb = shift(first_bottom, 1)
    row_rt = shift(first_top, -1)
    row_ft = shift(row_lt, 1)
    row_fb = shift(row_rb, -1)
    left_top, right_bottom, *held = feed_forward((row_lt, row_rb), (weights,))
    left_plain = shift(right_bottom, 1)
    right_plain = shift(left_top, -1)
    far_top, far_bottom = feed_forward((row_ft, row_fb), held)
    from_left = shift(far_top, 1)
    from_right = shift(far_bottom, -1)
    left_bottom, right_top = feed_forward((row_lb, row_rt), held)
    left_sum = shift(added(right_top, from_left), 1)
    right_sum = shift(added(left_bottom, from_right), -1)
    own_top, own_bottom = feed_forward((first_top, first_bottom), held)
    out = norm_half(
        (first_top, own_top, left_sum, right_plain), 0, norm2_gain, norm2_bias, half, rows
    )
    return norm_half(
        (first_bottom, own_bottom, left_plain, right_sum),
        half,
        norm2_gain,
        norm2_bias,
        half,
        rows,
        out,
    )


def solution(mesh):
    return jax.shard_map(
        layer,
        mesh=mesh,
        in_specs=(
            P(("sp", "tp"), None),
            P("sp", "tp"),
            P(None, "sp", "tp"),
            P("tp"),
            P("tp", None),
            P(),
            P(),
            P("sp", "tp"),
            P("tp", "sp"),
            P(),
            P(),
        ),
        out_specs=P(("sp", "tp"), None),
        check_vma=False,
    )
```
